1024 devices in a mesh: sp: 16 (over x, core), dp: 64 (over z, y).
Axes of the slice: x: 8, y: 8, z: 8, core: 2. Of those that a mesh axis runs over, the one named last changes fastest.
Arguments:
- content_features_raw: bfloat16 [64, 2048, 3072], P('dp', 'sp'), may hold values from -6 to 6
- memory_entering_matrix: bfloat16 [64, 2048, 2048], P('dp', 'sp'), may hold values from -6 to 6
- memory_leaving_matrix: bfloat16 [64, 2048, 2048], P('dp', 'sp'), may hold values from -6 to 6
- feature_switch_signal: bfloat16 [64, 2048, 3072], P('dp', 'sp'), may hold values from -6 to 6
- ahead_increment_raw: float32 [64, 2048, 48], P('dp', 'sp'), may hold values from -5 to 5
- reverse_increment_raw: float32 [64, 2048, 48], P('dp', 'sp'), may hold values from -5 to 5
- additional_fading: float32 [64, 2048, 48], P('dp', 'sp'), as said below
- content_filter_weights: bfloat16 [4, 3072], P(None, 'sp'), may hold values from -3 to 3
- entering_filter_weights: bfloat16 [4, 2048], P(None, 'sp'), may hold values from -3 to 3
- leaving_filter_weights: bfloat16 [4, 2048], P(None, 'sp'), may hold values from -3 to 3
- increment_offset_lanes: float32 [2, 48], P(None, 'sp'), may hold values from -0.5 to 0.5
- fading_speed_exponents: float32 [2, 48], P(None, 'sp'), as said below
- result_scaling_factor: bfloat16 [3072], replicated, may hold values from 0.099609375 to 1.8984375
Outputs:
- out: bfloat16 [64, 2048, 3072], P('dp', 'sp')
The draws below stay inside these ranges and needn't reach their ends.
Inputs may be any that keep to these rules, and one draw needn't show every extreme that they name: Each head's row has a rate exp(fading_speed_exponents) between 0.3 / 131072 and 0.05. `additional_fading`: zero at most positions; elsewhere between log(0.5) and log(0.8).
All inputs are finite; a program needn't handle non-finite values.
Results may differ from the reference program's by a relative error of at most 0.0051.
Values may be sent and summed in bfloat16 or wider, within the bound.
A program may use at most 64 MiB of HBM per device.

```python
import math
import jax
import jax.numpy as jnp
from jax import lax

ATTENTION_LANES = 48
HEAD_DIM = 64
GROUPS = 16
STATE = 128
TAPS = 4
BLK = 128
TOK_DEV = 128
SEGMENTS = 64
SEG_LEN = 2048
SEQ_LEN = 131072
D_SSM = 3072


def draw_fading_speed_exponents(key, part):
    first_key, second_key, third_key = jax.random.split(key, 3)
    share = 0.5
    slow_pick = jax.random.uniform(first_key, (2, ATTENTION_LANES), jnp.float32) < share
    slow_low = math.log(0.3 / SEQ_LEN)
    slow_high = math.log(min(2.0 / SEG_LEN, 0.015))
    slow_rate = jax.random.uniform(second_key, (2, ATTENTION_LANES), jnp.float32, slow_low, slow_high)
    fast_rate = jax.random.uniform(third_key, (2, ATTENTION_LANES), jnp.float32, math.log(0.015), math.log(0.05))
    return jnp.where(slow_pick, slow_rate, fast_rate).astype(jnp.float32)


def step_rates(key, salt):
    folded = jax.random.fold_in(key, salt)
    first_key, second_key = jax.random.split(folded)
    block_count = SEQ_LEN // TOK_DEV
    noise_draw = jnp.clip(jax.random.normal(first_key, (block_count, TOK_DEV, ATTENTION_LANES), jnp.float32), -3.0, 3.0)
    offset = jax.random.uniform(second_key, (block_count, 1, ATTENTION_LANES), jnp.float32, -1.2, 1.2)
    return (noise_draw + offset).reshape(SEGMENTS, SEG_LEN, ATTENTION_LANES).astype(jnp.float32)


def draw_ahead_increment_raw(key, part):
    return step_rates(key, 11)


def draw_reverse_increment_raw(key, part):
    return step_rates(key, 23)


def draw_additional_fading(key, part):
    first_key, second_key = jax.random.split(key)
    struck = jax.random.uniform(first_key, (SEGMENTS, SEG_LEN, ATTENTION_LANES), jnp.float32) < 3.0 / SEQ_LEN
    loss_log = jnp.log(jax.random.uniform(second_key, (SEGMENTS, SEG_LEN, ATTENTION_LANES), jnp.float32, 0.5, 0.8))
    return jnp.where(struck, loss_log, 0.0).astype(jnp.float32)


def levels(rng, extent, cuts, low, largest):
    def one(position, shards_of):
        steps = jax.random.uniform(jax.random.fold_in(jax.random.fold_in(rng, 6), position), (shards_of,), jnp.float32, low / len(cuts), largest / len(cuts))
        return jnp.repeat(jnp.exp(steps), extent[position] // shards_of).reshape((-1,) + (1,) * (len(extent) - position - 1))

    level = one(*cuts[0])
    for cut in cuts[1:]:
        level = level * one(*cut)
    return level


def gaussian(stream_key, extent, spread, limit, shards=(), kind=jnp.bfloat16):
    values = jax.random.normal(stream_key, extent, jnp.float32) * spread
    if len(shards) > 0:
        values = levels(stream_key, extent, shards, -0.22, 0.18) * values
    return jnp.clip(values, min=-limit, max=limit).astype(kind)


def setup_inputs(seed: int = 0) -> dict:
    streams_of = jax.random.split(jax.random.key(seed), 14)
    content_features_raw = gaussian(streams_of[0], (SEGMENTS, SEG_LEN, D_SSM), 1.0, 6.0, ((0, 64), (1, 16)))
    memory_entering_matrix = gaussian(streams_of[1], (SEGMENTS, SEG_LEN, GROUPS * STATE), 1.0, 6.0, ((0, 64), (1, 16)))
    memory_leaving_matrix = gaussian(streams_of[2], (SEGMENTS, SEG_LEN, GROUPS * STATE), 1.0, 6.0, ((0, 64), (1, 16)))
    feature_switch_signal = gaussian(streams_of[3], (SEGMENTS, SEG_LEN, D_SSM), 1.0, 6.0, ((0, 64), (1, 16)))
    ahead_increment_raw = draw_ahead_increment_raw(jax.random.fold_in(streams_of[13], 71), 0)
    reverse_increment_raw = draw_reverse_increment_raw(jax.random.fold_in(streams_of[13], 71), 0)
    additional_fading = draw_additional_fading(jax.random.fold_in(streams_of[13], 71), 0)
    content_filter_weights = gaussian(streams_of[7], (TAPS, D_SSM), TAPS ** -0.5, 3.0, ((1, 16),))
    entering_filter_weights = gaussian(streams_of[8], (TAPS, GROUPS * STATE), TAPS ** -0.5, 3.0, ((1, 16),))
    leaving_filter_weights = gaussian(streams_of[9], (TAPS, GROUPS * STATE), TAPS ** -0.5, 3.0, ((1, 16),))
    increment_offset_lanes = jnp.clip(jax.random.uniform(streams_of[10], (2, ATTENTION_LANES), jnp.float32, -0.5, 0.5) * levels(streams_of[10], (2, ATTENTION_LANES), ((1, 16),), -0.4, 0.0), -0.5, 0.5)
    fading_speed_exponents = draw_fading_speed_exponents(jax.random.fold_in(streams_of[13], 71), 0)
    result_scaling_factor = jnp.clip(1.0 + 0.18 * jax.random.normal(streams_of[12], (D_SSM,), jnp.float32), 0.099609375, 1.8984375).astype(jnp.bfloat16)
    return {"content_features_raw": content_features_raw, "memory_entering_matrix": memory_entering_matrix, "memory_leaving_matrix": memory_leaving_matrix, "feature_switch_signal": feature_switch_signal, "ahead_increment_raw": ahead_increment_raw, "reverse_increment_raw": reverse_increment_raw, "additional_fading": additional_fading, "content_filter_weights": content_filter_weights, "entering_filter_weights": entering_filter_weights, "leaving_filter_weights": leaving_filter_weights, "increment_offset_lanes": increment_offset_lanes, "fading_speed_exponents": fading_speed_exponents, "result_scaling_factor": result_scaling_factor}


def conv_silu(padded, weight, length):
    total_sum = padded[0:length].astype(jnp.float32) * weight[0].astype(jnp.float32)
    for lag_step in range(1, weight.shape[0]):
        total_sum = total_sum + padded[lag_step:lag_step + length].astype(jnp.float32) * weight[lag_step].astype(jnp.float32)
    return jax.nn.silu(total_sum).astype(jnp.bfloat16)

def direction(x_conv, b_conv, c_conv, rate, log_decay):
    overall_position_count = x_conv.shape[0]
    heads_within_group = rate.shape[1]
    block_count = overall_position_count // BLK
    x_blocks = x_conv.reshape(block_count, BLK, heads_within_group, HEAD_DIM)
    b_blocks = b_conv.reshape(block_count, BLK, STATE)
    c_blocks = c_conv.reshape(block_count, BLK, STATE)
    rate_blocks = rate.reshape(block_count, BLK, heads_within_group)
    log_blocks = log_decay.reshape(block_count, BLK, heads_within_group)
    lower_mask = jnp.tril(jnp.ones((BLK, BLK), bool))[:, :, None]

    def step(state, pieces):
        x_block, b_block, c_block, rate_block, log_block = pieces
        cum_log = jnp.cumsum(log_block, axis=0)
        scores = jnp.dot(c_block, b_block.T, preferred_element_type=jnp.float32)
        log_gaps = jnp.where(lower_mask, cum_log[:, None, :] - cum_log[None, :, :], -jnp.inf)
        weights = (scores[:, :, None] * jnp.exp(log_gaps) * rate_block[None, :, :]).astype(jnp.bfloat16)
        local_part = jnp.einsum('lsh,shp->lhp', weights.astype(jnp.float32), x_block.astype(jnp.float32))
        carried_part = jnp.einsum('ln,hpn->lhp', c_block.astype(jnp.float32), state, precision=lax.Precision.HIGHEST) * jnp.exp(cum_log)[:, :, None]
        block_log = cum_log[-1]
        scaled = (x_block.astype(jnp.float32) * (rate_block * jnp.exp(block_log[None, :] - cum_log))[:, :, None]).astype(jnp.bfloat16)
        update = jnp.einsum('shp,sn->hpn', scaled.astype(jnp.float32), b_block.astype(jnp.float32))
        new_state = state * jnp.exp(block_log)[:, None, None] + update
        return (new_state, local_part + carried_part)
    initial = jnp.zeros((heads_within_group, HEAD_DIM, STATE), jnp.float32)
    _, outputs = lax.scan(step, initial, (x_blocks, b_blocks, c_blocks, rate_blocks, log_blocks))
    return outputs.reshape(overall_position_count, heads_within_group * HEAD_DIM)

def reference(content_features_raw, memory_entering_matrix, memory_leaving_matrix, feature_switch_signal, ahead_increment_raw, reverse_increment_raw, additional_fading, content_filter_weights, entering_filter_weights, leaving_filter_weights, increment_offset_lanes, fading_speed_exponents, result_scaling_factor):
    overall_position_count = SEGMENTS * SEG_LEN
    width = ATTENTION_LANES * HEAD_DIM
    heads_within_group = ATTENTION_LANES // GROUPS
    group_width = heads_within_group * HEAD_DIM
    x_flat = content_features_raw.reshape(overall_position_count, width)
    b_flat = memory_entering_matrix.reshape(overall_position_count, GROUPS * STATE)
    c_flat = memory_leaving_matrix.reshape(overall_position_count, GROUPS * STATE)
    z_flat = feature_switch_signal.reshape(overall_position_count, width)
    fwd_flat = ahead_increment_raw.reshape(overall_position_count, ATTENTION_LANES)
    bwd_flat = reverse_increment_raw.reshape(overall_position_count, ATTENTION_LANES)
    additional_fading_flat_array = additional_fading.reshape(overall_position_count, ATTENTION_LANES)

    def one_group(group):
        col_x = (group * group_width).astype(jnp.int32)
        col_b = (group * STATE).astype(jnp.int32)
        column_per_head = (group * heads_within_group).astype(jnp.int32)
        x_part = lax.dynamic_slice_in_dim(x_flat, col_x, group_width, 1)
        b_part = lax.dynamic_slice_in_dim(b_flat, col_b, STATE, 1)
        c_part = lax.dynamic_slice_in_dim(c_flat, col_b, STATE, 1)
        z_part = lax.dynamic_slice_in_dim(z_flat, col_x, group_width, 1)
        pad_rows = ((2, TAPS - 3), (0, 0))
        x_conv = conv_silu(jnp.pad(x_part, pad_rows), lax.dynamic_slice_in_dim(content_filter_weights, col_x, group_width, 1), overall_position_count)
        b_conv = conv_silu(jnp.pad(b_part, pad_rows), lax.dynamic_slice_in_dim(entering_filter_weights, col_b, STATE, 1), overall_position_count)
        c_conv = conv_silu(jnp.pad(c_part, pad_rows), lax.dynamic_slice_in_dim(leaving_filter_weights, col_b, STATE, 1), overall_position_count)
        bias_part = lax.dynamic_slice_in_dim(increment_offset_lanes, column_per_head, heads_within_group, 1)
        decay_log_piece = lax.dynamic_slice_in_dim(fading_speed_exponents, column_per_head, heads_within_group, 1)
        spike_piece = lax.dynamic_slice_in_dim(additional_fading_flat_array, column_per_head, heads_within_group, 1)
        forward_step_rate = jax.nn.softplus(lax.dynamic_slice_in_dim(fwd_flat, column_per_head, heads_within_group, 1) + bias_part[0])
        backward_step_rate = jax.nn.softplus(lax.dynamic_slice_in_dim(bwd_flat, column_per_head, heads_within_group, 1) + bias_part[1])
        forward_log_decay = -jnp.exp(decay_log_piece[0]) * forward_step_rate + spike_piece
        backward_log_decay = -jnp.exp(decay_log_piece[1]) * backward_step_rate + spike_piece
        y_fwd = direction(x_conv, b_conv, c_conv, forward_step_rate, forward_log_decay)
        y_bwd = direction(x_conv[::-1], b_conv[::-1], c_conv[::-1], backward_step_rate[::-1], backward_log_decay[::-1])[::-1]
        mixed = (y_fwd + y_bwd).astype(jnp.bfloat16)
        gated = mixed.astype(jnp.float32) * jax.nn.silu(z_part.astype(jnp.float32))
        by_head = gated.reshape(overall_position_count, heads_within_group, HEAD_DIM)
        normed = by_head * lax.rsqrt(lax.optimization_barrier(jnp.mean(by_head * by_head, axis=-1, keepdims=True)) + 1e-06)
        gain_part = lax.dynamic_slice_in_dim(result_scaling_factor, col_x, group_width, 0).astype(jnp.float32)
        return (normed.reshape(overall_position_count, group_width) * gain_part).astype(jnp.bfloat16)
    results = lax.map(one_group, jnp.arange(GROUPS, dtype=jnp.int32))
    return jnp.transpose(results, (1, 0, 2)).reshape(SEGMENTS, SEG_LEN, width)
```

```python
import functools

import jax
import jax.numpy as jnp
from jax import lax
from jax.experimental import pallas as pl
from jax.experimental.pallas import tpu as pltpu
from jax.sharding import Mesh
from jax.sharding import PartitionSpec as P

MESH = pl.DeviceIdType.MESH
HEAD_DIM = 64
STATE = 128
TOK = 128
HPG = 3
GW = HPG * HEAD_DIM
PW = 2 * GW
HIGH = lax.Precision.HIGHEST
F32 = jnp.float32
BF16 = jnp.bfloat16


def iota(shape, dim):
    return lax.broadcasted_iota(jnp.int32, shape, dim)


def mm(a, b, precision=None):
    return jnp.dot(a, b, preferred_element_type=F32, precision=precision)


def rcopy(src, dst, send_sem, recv_sem, device):
    return pltpu.make_async_remote_copy(
        src_ref=src,
        dst_ref=dst,
        send_sem=send_sem,
        recv_sem=recv_sem,
        device_id=device,
        device_id_type=MESH,
    )


def expand(columns, ids):
    low = iota((columns.shape[0], 128), 1) < HEAD_DIM
    pieces = []
    for v in range(len(ids) // 2):
        a, b = ids[2 * v], ids[2 * v + 1]
        pieces.append(jnp.where(low, columns[:, a : a + 1], columns[:, b : b + 1]))
    return jnp.concatenate(pieces, axis=1)


def group_ids(q):
    return [HPG * q + i for i in range(HPG)] + [8 + HPG * q + i for i in range(HPG)]


def conv_silu(own, other, before, after, taps, first):
    own, other = own.astype(F32), other.astype(F32)
    x = jnp.concatenate(
        [jnp.where(first, own, other), jnp.where(first, other, own)], axis=0
    )
    rows = x.shape[0]
    row = iota(x.shape, 0)
    m1 = jnp.where(row == 0, before[1:2], pltpu.roll(x, 1, 0))
    m2 = jnp.where(
        row == 0, before[0:1], jnp.where(row == 1, before[1:2], pltpu.roll(x, 2, 0))
    )
    p1 = jnp.where(row == rows - 1, after[0:1], pltpu.roll(x, rows - 1, 0))
    total = m2 * taps[0:1] + m1 * taps[1:2] + x * taps[2:3] + p1 * taps[3:4]
    return (total / (1.0 + jnp.exp(-total))).astype(BF16)


def kernel(
    sizes,
    x_ref, b_ref, c_ref, z_ref, ra_ref, rr_ref, rf_ref,
    wx_ref, wb_ref, wc_ref, off_ref, spd_ref, gain_ref,
    out_ref,
    xo, bo, co, ro, hs, hr, ws, wr,
    cum_t, rate_t, fac_t, ecum_t,
    xc, bc, cc, yl,
    ts, tr, ls, lr, pre, pcl,
    ss, sl, yr, ylr, ypre, ypcl,
    zq, zql, zr, zlr,
    isd, ir, es, er,
    ys, yx,
    d_s, d_r, h_s, h_r, w_s, w_r,
    t_s, t_r, l_s, l_r, s_s, s_r, sl_s, sl_r,
    q_s, q_r, ql_s, ql_r, i_s, i_r, e_s, e_r, y_s, y_r,
):
    nx, ny, nz = sizes
    pairs = nx // 2
    xw, bw = pairs * PW, pairs * 2 * STATE
    x, c, z, y = (lax.axis_index(n) for n in ("x", "c", "z", "y"))
    first = c == 0
    partner = {"c": 1 - c}
    lin = (z * ny + y) * nx + x
    total_chips = nx * ny * nz
    has_prev, has_next = lin > 0, lin < total_chips - 1

    def chip(at):
        at = lax.rem(at + total_chips, total_chips)
        rest = at // nx
        return {"x": lax.rem(at, nx), "y": lax.rem(rest, ny), "z": rest // ny}

    target_exists = jnp.logical_or(
        jnp.logical_and(first, has_prev), jnp.logical_and(jnp.logical_not(first), has_next)
    )
    target = chip(jnp.where(first, lin - 1, lin + 1))

    barrier = pltpu.get_barrier_semaphore()

    def greet(device):
        pl.semaphore_signal(barrier, inc=1, device_id=device, device_id_type=MESH)

    greet(partner)

    @pl.loop(1, nx)
    def _(k):
        at = lax.rem(x + k, nx)
        greet({"x": at})
        greet({"x": at, "c": 1 - c})

    @pl.loop(1, ny)
    def _(k):
        greet({"y": lax.rem(y + k, ny)})

    @pl.loop(1, nz)
    def _(k):
        greet({"z": lax.rem(z + k, nz)})

    @pl.when(has_prev)
    def _():
        greet({**chip(lin - 1), "c": 1})

    @pl.when(has_next)
    def _():
        greet({**chip(lin + 1), "c": 0})

    group = 2 * x + c
    slot = lax.rem(group, nx)
    parity = lax.rem(slot, 2)
    place = (iota((GW, PW), 1) == iota((GW, PW), 0) + GW * parity).astype(BF16)
    ws[0:4, 0:PW] = mm(wx_ref[...], place)
    ws[0:4, PW : PW + STATE] = wb_ref[...].astype(F32)
    ws[0:4, PW + STATE : PW + 2 * STATE] = wc_ref[...].astype(F32)
    lane = iota((1, 128), 1)
    base = 16 * (slot // 2) + HPG * parity
    offsets = jnp.zeros((1, 128), F32)
    speeds = jnp.zeros((1, 128), F32)
    for d in range(2):
        for i in range(HPG):
            here = lane == base + 8 * d + i
            offsets = jnp.where(here, off_ref[d : d + 1, i : i + 1], offsets)
            speeds = jnp.where(here, spd_ref[d : d + 1, i : i + 1], speeds)
    ws[4:5, 0:128] = offsets
    ws[5:6, 0:128] = speeds

    at = 0
    for ref, width in ((x_ref, xw), (b_ref, bw), (c_ref, bw)):
        for half in range(2):
            cols = pl.ds(half * width, width)
            last = ref[0, TOK - 16 : TOK, cols].astype(F32)[8:16]
            start = ref[0, 0:16, cols].astype(F32)[0:8]
            rows = jnp.where(first, start, pltpu.roll(last, 2, 0))
            hs[half, :, at : at + width] = rows[0:2]
        at += width

    @pl.when(jnp.logical_not(has_prev))
    def _():
        hr[0] = jnp.zeros(hr.shape[1:], F32)

    @pl.when(jnp.logical_not(has_next))
    def _():
        hr[1] = jnp.zeros(hr.shape[1:], F32)

    expected = 1 + 2 * (nx - 1) + (ny - 1) + (nz - 1)
    pl.semaphore_wait(barrier, expected + jnp.where(target_exists, 2, 0))

    def half_of(ref, width, half):
        return ref.at[0, :, pl.ds(pl.multiple_of(half * width, 128), width)]

    rate_copies = [
        rcopy(ref.at[0], ro.at[k], d_s.at[k], d_r.at[k], partner)
        for k, ref in enumerate((ra_ref, rr_ref, rf_ref))
    ]
    data_copies = [
        rcopy(half_of(ref, width, 1 - c), dst, d_s.at[3 + k], d_r.at[3 + k], partner)
        for k, (ref, width, dst) in enumerate(((x_ref, xw, xo), (b_ref, bw, bo), (c_ref, bw, co)))
    ]
    for copy in rate_copies:
        copy.start()

    to_core = group // nx

    def weight_copy(j):
        return rcopy(ws, wr.at[slot], w_s.at[j], w_r.at[slot], {"x": j, "c": to_core})

    def weight_is_mine(j):
        return jnp.logical_and(j == x, to_core == c)

    @pl.loop(0, nx)
    def _(k):
        j = lax.rem(x + k, nx)

        @pl.when(jnp.logical_not(weight_is_mine(j)))
        def _():
            weight_copy(j).start()

    @pl.when(to_core == c)
    def _():
        wr[slot] = ws[...]

    def halo_copy(half):
        return rcopy(
            hs.at[half], hr.at[1 - c], h_s.at[half], h_r.at[1 - c], {**target, "c": half}
        )

    @pl.when(target_exists)
    def _():
        for half in range(2):
            halo_copy(half).start()

    for copy in data_copies:
        copy.start()

    for copy in rate_copies:
        copy.wait_recv()

    @pl.loop(0, nx)
    def _(j):
        @pl.when(jnp.logical_not(nx * c + j == group))
        def _():
            rcopy(ws, wr.at[j], w_s.at[j], w_r.at[j], partner).wait_recv()

    heads = ra_ref.shape[2]
    head, lanes = iota((heads, 128), 0), iota((heads, 128), 1)
    pair, rest = lanes // 16, lax.rem(lanes, 16)
    inside = lax.rem(rest, 8)
    valid = jnp.logical_and(inside < 6, pair < pairs)
    valid = jnp.logical_and(valid, head == 6 * pairs * c + 6 * pair + inside)
    pick_f = jnp.logical_and(valid, rest < 8).astype(F32)
    pick_b = jnp.logical_and(valid, rest >= 8).astype(F32)

    def both(ref, k):
        own, other = ref[0], ro[k]
        return jnp.concatenate(
            [jnp.where(first, own, other), jnp.where(first, other, own)], axis=0
        )

    raw = mm(both(ra_ref, 0), pick_f, HIGH) + mm(both(rr_ref, 1), pick_b, HIGH)
    fading = mm(both(rf_ref, 2), pick_f + pick_b, HIGH)
    offset_row = wr[0, 4:5, 0:128]
    speed_row = wr[0, 5:6, 0:128]
    for j in range(1, nx):
        offset_row = offset_row + wr[j, 4:5, 0:128]
        speed_row = speed_row + wr[j, 5:6, 0:128]
    pre_rate = raw + offset_row
    rate = jnp.maximum(pre_rate, 0.0) + jnp.log1p(jnp.exp(-jnp.abs(pre_rate)))
    log = fading - jnp.exp(speed_row) * rate
    n = 2 * TOK
    row_i, col_i = iota((n, n), 0), iota((n, n), 1)
    forward = lax.rem(iota((1, 128), 1), 16) < 8
    cum = jnp.where(
        forward,
        mm((col_i <= row_i).astype(F32), log, HIGH),
        mm((col_i >= row_i).astype(F32), log, HIGH),
    )
    span = jnp.where(forward, cum[n - 1 : n], cum[0:1])
    cum_t[...] = cum.T
    rate_t[...] = rate.T
    fac_t[...] = (rate * jnp.exp(span - cum)).T
    ecum_t[...] = jnp.exp(cum).T

    @pl.when(has_prev)
    def _():
        rcopy(hs.at[0], hr.at[0], h_s.at[0], h_r.at[0], partner).wait_recv()

    @pl.when(has_next)
    def _():
        rcopy(hs.at[0], hr.at[1], h_s.at[0], h_r.at[1], partner).wait_recv()

    for copy in data_copies:
        copy.wait_recv()

    half_lane = iota((1, PW), 1) < GW

    def rows_of(p):
        return pl.ds(pl.multiple_of(16 * p, 16), 16)

    def x_cols(p):
        return pl.ds(pl.multiple_of(PW * p, 128), PW)

    def b_cols(p):
        return pl.ds(pl.multiple_of(2 * STATE * p, 128), 2 * STATE)

    def state_copy(j):
        return rcopy(ts.at[j], tr.at[x], t_s.at[j], t_r.at[x], {"x": j})

    def log_copy(j):
        return rcopy(ls.at[j], lr.at[x], l_s.at[j], l_r.at[x], {"x": j})

    @pl.loop(0, pairs)
    def _(k):
        p = lax.rem(x // 2 + 1 + k, pairs)
        w0, w1 = wr[2 * p], wr[2 * p + 1]
        cols, start = x_cols(p), pl.multiple_of(PW * p, 128)
        x_cols_in = pl.ds(pl.multiple_of(c * xw + start, 128), PW)
        xv = conv_silu(
            x_ref[0, :, x_cols_in], xo[:, cols], hr[0, :, cols], hr[1, :, cols],
            w0[0:4, 0:PW] + w1[0:4, 0:PW], first,
        )
        xc[:, cols] = xv
        convs = []
        for own, other, dst, at, lo in ((b_ref, bo, bc, xw, PW), (c_ref, co, cc, xw + bw, PW + STATE)):
            start = pl.multiple_of(2 * STATE * p, 128)
            taps = jnp.concatenate([w0[0:4, lo : lo + STATE], w1[0:4, lo : lo + STATE]], axis=1)
            cols_in = pl.ds(pl.multiple_of(c * bw + start, 128), 2 * STATE)
            cols_h = pl.ds(pl.multiple_of(at + start, 128), 2 * STATE)
            v = conv_silu(
                own[0, :, cols_in], other[:, b_cols(p)], hr[0, :, cols_h], hr[1, :, cols_h],
                taps, first,
            )
            dst[:, b_cols(p)] = v
            convs.append(v)
        factors = fac_t[rows_of(p)].T
        cums = cum_t[rows_of(p)].T
        direction = iota((1, 16), 1) < 8
        spans = jnp.where(direction, cums[n - 1 : n], cums[0:1])
        xf = xv.astype(F32)
        swapped = pltpu.roll(xf, GW, 1)
        bf = convs[0].astype(F32)
        for q in range(2):
            j = 2 * p + q
            twice = jnp.where(half_lane, xf, swapped) if q == 0 else jnp.where(half_lane, swapped, xf)
            scaled = twice * expand(factors, group_ids(q))
            hi = scaled.astype(BF16)
            lo = (scaled - hi.astype(F32)).astype(BF16)
            bt = bf[:, q * STATE : (q + 1) * STATE].T.astype(BF16)
            update = (mm(bt, hi) + mm(bt, lo)).astype(BF16)
            span_row = expand(spans, group_ids(q))

            @pl.when(j == x)
            def _():
                tr[x] = update
                lr[x] = span_row

            @pl.when(j != x)
            def _():
                ls[j] = span_row
                ts[j] = update
                log_copy(j).start()
                state_copy(j).start()

    @pl.loop(0, pairs)
    def _(p):
        cum_r, rate_r = cum_t[rows_of(p)], rate_t[rows_of(p)]
        cum_c = cum_r.T
        xv, bv, cv = xc[:, x_cols(p)], bc[:, b_cols(p)], cc[:, b_cols(p)]
        below, above = col_i < row_i, col_i > row_i
        low = iota((n, 128), 1) < HEAD_DIM
        products = []
        for q in range(2):
            scores = lax.dot_general(
                cv[:, q * STATE : (q + 1) * STATE], bv[:, q * STATE : (q + 1) * STATE],
                (((1,), (1,)), ((), ())), preferred_element_type=F32,
            )
            for i in range(HPG):
                f, g = HPG * q + i, 8 + HPG * q + i
                gap = jnp.where(
                    above,
                    cum_c[:, g : g + 1] - cum_r[g : g + 1],
                    cum_c[:, f : f + 1] - cum_r[f : f + 1],
                )
                r_f, r_b = rate_r[f : f + 1], rate_r[g : g + 1]
                coef = jnp.where(below, r_f, jnp.where(above, r_b, r_f + r_b))
                weights = (scores * jnp.exp(gap) * coef).astype(BF16)
                v = f // 2
                products.append(mm(weights, xv[:, 128 * v : 128 * (v + 1)]))
        yl[:, x_cols(p)] = jnp.concatenate(
            [jnp.where(low, products[2 * v], products[2 * v + 1]) for v in range(HPG)], axis=1
        )

    @pl.loop(0, nx)
    def _(k):
        @pl.when(k != x)
        def _():
            rcopy(ls.at[k], lr.at[k], l_s.at[k], l_r.at[k], partner).wait_recv()
            rcopy(ts.at[k], tr.at[k], t_s.at[k], t_r.at[k], partner).wait_recv()

    pre[0] = jnp.zeros(pre.shape[1:], F32)
    pcl[0] = jnp.zeros(pcl.shape[1:], F32)

    @pl.loop(0, nx)
    def _(k):
        d = jnp.where(half_lane, lr[k], lr[nx - 1 - k])
        v = jnp.where(half_lane, tr[k], tr[nx - 1 - k]).astype(F32)
        pre[k + 1] = pre[k] * jnp.exp(d) + v
        pcl[k + 1] = pcl[k] + d

    ry = STATE // ny

    def y_rows(j):
        return pl.ds(pl.multiple_of(ry * j, ry), ry)

    ss[...] = pre[nx].astype(ss.dtype)
    sl[...] = pcl[nx]

    @pl.loop(1, ny)
    def _(k):
        j = lax.rem(y + k, ny)
        rcopy(sl, ylr.at[y], sl_s.at[j], sl_r.at[y], {"y": j}).start()
        rcopy(ss.at[y_rows(j)], yr.at[y], s_s.at[j], s_r.at[y], {"y": j}).start()

    yr[y] = ss[y_rows(y)]
    ylr[y] = sl[...]

    @pl.loop(1, ny)
    def _(k):
        j = lax.rem(y + k, ny)
        rcopy(sl, ylr.at[j], sl_s.at[j], sl_r.at[j], {"y": j}).wait_recv()
        rcopy(ss.at[y_rows(j)], yr.at[j], s_s.at[j], s_r.at[j], {"y": j}).wait_recv()

    ypre[0] = jnp.zeros(ypre.shape[1:], F32)
    ypcl[0] = jnp.zeros(ypcl.shape[1:], F32)

    @pl.loop(0, ny)
    def _(k):
        d = jnp.where(half_lane, ylr[k], ylr[ny - 1 - k])
        v = jnp.where(half_lane, yr[k].astype(F32), yr[ny - 1 - k].astype(F32))
        ypre[k + 1] = ypre[k] * jnp.exp(d) + v
        ypcl[k + 1] = ypcl[k] + d

    zq[...] = ypre[ny]
    zql[...] = ypcl[ny]

    @pl.loop(1, nz)
    def _(k):
        j = lax.rem(z + k, nz)
        rcopy(zql, zlr.at[z], ql_s.at[j], ql_r.at[z], {"z": j}).start()
        rcopy(zq, zr.at[z], q_s.at[j], q_r.at[z], {"z": j}).start()

    zr[z] = zq[...]
    zlr[z] = zql[...]

    @pl.loop(1, nz)
    def _(k):
        j = lax.rem(z + k, nz)
        rcopy(zql, zlr.at[j], ql_s.at[j], ql_r.at[j], {"z": j}).wait_recv()
        rcopy(zq, zr.at[j], q_s.at[j], q_r.at[j], {"z": j}).wait_recv()

    running = jnp.zeros((ry, PW), F32)
    entering = jnp.zeros((ry, PW), F32)
    wanted = jnp.where(half_lane, z, nz - 1 - z)
    for k in range(nz):
        entering = jnp.where(wanted == k, running, entering)
        d = jnp.where(half_lane, zlr[k], zlr[nz - 1 - k])
        v = jnp.where(half_lane, zr[k], zr[nz - 1 - k])
        running = running * jnp.exp(d) + v

    def incoming(k):
        return ypre[k] + jnp.exp(ypcl[k]) * entering

    @pl.loop(1, ny)
    def _(k):
        j = lax.rem(y + k, ny)
        isd[j] = jnp.where(half_lane, incoming(j), incoming(ny - 1 - j)).astype(isd.dtype)
        rcopy(isd.at[j], ir.at[y_rows(y)], i_s.at[j], i_r.at[y], {"y": j}).start()

    ir[y_rows(y)] = jnp.where(half_lane, incoming(y), incoming(ny - 1 - y)).astype(ir.dtype)

    @pl.loop(1, ny)
    def _(k):
        j = lax.rem(y + k, ny)
        rcopy(isd.at[j], ir.at[y_rows(j)], i_s.at[j], i_r.at[j], {"y": j}).wait_recv()

    def entry(j):
        here = ir[...].astype(F32)
        f = pre[j] + jnp.exp(pcl[j]) * here
        b = pre[nx - 1 - j] + jnp.exp(pcl[nx - 1 - j]) * here
        return jnp.where(half_lane, f, b).astype(BF16)

    @pl.loop(1, nx)
    def _(k):
        j = lax.rem(x + k, nx)
        es[j] = entry(j)
        rcopy(es.at[j], er.at[x], e_s.at[j], e_r.at[x], {"x": j}).start()

    er[x] = entry(x)

    block_r, block_c = iota((128, 128), 0) // HEAD_DIM, iota((128, 128), 1) // HEAD_DIM
    ones = (block_r == block_c).astype(BF16)

    def gate(mixed, cols):
        zz = z_ref[0, :, cols].astype(F32)
        g = mixed.astype(F32) * (zz / (1.0 + jnp.exp(-zz)))
        sq = g * g
        hi = sq.astype(BF16)
        lo = (sq - hi.astype(F32)).astype(BF16)
        means = jnp.concatenate(
            [
                mm(hi[:, 128 * v : 128 * (v + 1)], ones) + mm(lo[:, 128 * v : 128 * (v + 1)], ones)
                for v in range(HPG)
            ],
            axis=1,
        ) * (1.0 / HEAD_DIM)
        normed = g * lax.rsqrt(means + 1e-06)
        out_ref[0, :, cols] = (normed * gain_ref[:, cols].astype(F32)).astype(BF16)

    def own_cols(p, half):
        return pl.ds(pl.multiple_of(half * xw + PW * p, 128), PW)

    def mixed_copy(p):
        return rcopy(ys.at[p], yx.at[p], y_s.at[p], y_r.at[p], partner)

    @pl.loop(0, pairs)
    def _(k):
        p = lax.rem(x // 2 + k, pairs)
        cv = cc[:, b_cols(p)]
        decays = ecum_t[rows_of(p)].T
        carried = []
        for q in range(2):
            j = 2 * p + q

            @pl.when(j != x)
            def _():
                rcopy(es.at[j], er.at[j], e_s.at[j], e_r.at[j], partner).wait_recv()

            v = mm(cv[:, q * STATE : (q + 1) * STATE], er[j]) * expand(decays, group_ids(q))
            carried.append(v + pltpu.roll(v, GW, 1))
        mixed = yl[:, x_cols(p)] + jnp.where(half_lane, carried[0], carried[1])
        top, bottom = mixed[0:TOK].astype(BF16), mixed[TOK:n].astype(BF16)
        ys[p] = jnp.where(first, bottom, top)
        mixed_copy(p).start()
        gate(jnp.where(first, top, bottom), own_cols(p, c))

    @pl.loop(0, pairs)
    def _(k):
        p = lax.rem((x // 2) + k, pairs)
        mixed_copy(p).wait_recv()
        gate(yx[p], own_cols(p, 1 - c))

    for copy in rate_copies + data_copies:
        copy.wait_send()

    @pl.when(target_exists)
    def _():
        for half in range(2):
            halo_copy(half).wait_send()

    @pl.loop(0, nx)
    def _(j):
        @pl.when(jnp.logical_not(weight_is_mine(j)))
        def _():
            weight_copy(j).wait_send()

        @pl.when(j != x)
        def _():
            log_copy(j).wait_send()
            state_copy(j).wait_send()
            rcopy(es.at[j], er.at[x], e_s.at[j], e_r.at[x], {"x": j}).wait_send()

    @pl.loop(1, ny)
    def _(k):
        j = lax.rem(y + k, ny)
        rcopy(sl, ylr.at[y], sl_s.at[j], sl_r.at[y], {"y": j}).wait_send()
        rcopy(ss.at[y_rows(j)], yr.at[y], s_s.at[j], s_r.at[y], {"y": j}).wait_send()
        rcopy(isd.at[j], ir.at[y_rows(y)], i_s.at[j], i_r.at[y], {"y": j}).wait_send()

    @pl.loop(1, nz)
    def _(k):
        j = lax.rem(z + k, nz)
        rcopy(zql, zlr.at[z], ql_s.at[j], ql_r.at[z], {"z": j}).wait_send()
        rcopy(zq, zr.at[z], q_s.at[j], q_r.at[z], {"z": j}).wait_send()

    @pl.loop(0, pairs)
    def _(p):
        mixed_copy(p).wait_send()


def local(sizes, *args):
    nx, ny, nz = sizes
    pairs = nx // 2
    xw, bw = pairs * PW, pairs * 2 * STATE
    n = 2 * TOK
    ry = STATE // ny
    args = args[:-1] + (args[-1][None],)
    dma = pltpu.SemaphoreType.DMA
    vmem = pltpu.VMEM
    scratch = [
        vmem((TOK, xw), BF16), vmem((TOK, bw), BF16), vmem((TOK, bw), BF16),
        vmem((3, TOK, args[4].shape[2]), F32),
        vmem((2, 2, xw + 2 * bw), F32), vmem((2, 2, xw + 2 * bw), F32),
        vmem((8, PW + 2 * STATE), F32), vmem((nx, 8, PW + 2 * STATE), F32),
        vmem((128, n), F32), vmem((128, n), F32), vmem((128, n), F32), vmem((128, n), F32),
        vmem((n, xw), BF16), vmem((n, bw), BF16), vmem((n, bw), BF16), vmem((n, xw), F32),
        vmem((nx, STATE, PW), BF16), vmem((nx, STATE, PW), BF16),
        vmem((nx, 1, PW), F32), vmem((nx, 1, PW), F32),
        vmem((nx + 1, STATE, PW), F32), vmem((nx + 1, 1, PW), F32),
        vmem((STATE, PW), BF16), vmem((1, PW), F32),
        vmem((ny, ry, PW), BF16), vmem((ny, 1, PW), F32),
        vmem((ny + 1, ry, PW), F32), vmem((ny + 1, 1, PW), F32),
        vmem((ry, PW), F32), vmem((1, PW), F32),
        vmem((nz, ry, PW), F32), vmem((nz, 1, PW), F32),
        vmem((ny, ry, PW), BF16), vmem((STATE, PW), BF16),
        vmem((nx, STATE, PW), BF16), vmem((nx, STATE, PW), BF16),
        vmem((pairs, TOK, PW), BF16), vmem((pairs, TOK, PW), BF16),
    ]
    counts = [6, 6, 2, 2, nx, nx, nx, nx, nx, nx, ny, ny, ny, ny, nz, nz, nz, nz, ny, ny, nx, nx, pairs, pairs]
    scratch += [dma((k,)) for k in counts]
    return pl.pallas_call(
        functools.partial(kernel, sizes),
        out_shape=jax.ShapeDtypeStruct(args[0].shape, BF16),
        in_specs=[pl.BlockSpec(memory_space=pltpu.VMEM)] * len(args),
        out_specs=pl.BlockSpec(memory_space=pltpu.VMEM),
        scratch_shapes=scratch,
        compiler_params=pltpu.CompilerParams(
            collective_id=0, has_side_effects=True, vmem_limit_bytes=60 * 1024 * 1024
        ),
        name="mixer",
    )(*args)


def solution(mesh):
    sp, dp = mesh.shape["sp"], mesh.shape["dp"]
    nx = sp // 2
    ny = max(k for k in range(1, dp + 1) if dp % k == 0 and k * k <= dp)
    nz = dp // ny
    torus = Mesh(mesh.devices.reshape(nx, 2, nz, ny), ("x", "c", "z", "y"))
    rows = P(("z", "y"), ("x", "c"), None)
    cols = P(None, ("x", "c"))
    return jax.shard_map(
        functools.partial(local, (nx, ny, nz)),
        mesh=torus,
        in_specs=(rows,) * 7 + (cols,) * 5 + (P(),),
        out_specs=rows,
        check_vma=False,
    )
```

```python
import functools

import jax
import jax.numpy as jnp
from jax import lax
from jax.experimental import pallas as pl
from jax.experimental.pallas import tpu as pltpu
from jax.sharding import Mesh
from jax.sharding import PartitionSpec as P

MESH = pl.DeviceIdType.MESH
HEAD_DIM = 64
STATE = 128
TOK = 128
HPG = 3
TAPS = 4
GW = HPG * HEAD_DIM
PW = 2 * GW
HIGH = lax.Precision.HIGHEST
F32 = jnp.float32
BF16 = jnp.bfloat16


def iota(shape, dim):
    return lax.broadcasted_iota(jnp.int32, shape, dim)


def mm(a, b, precision=None):
    return jnp.dot(a, b, preferred_element_type=F32, precision=precision)


def rcopy(src, dst, send_sem, recv_sem, device):
    return pltpu.make_async_remote_copy(
        src_ref=src,
        dst_ref=dst,
        send_sem=send_sem,
        recv_sem=recv_sem,
        device_id=device,
        device_id_type=MESH,
    )


def head_rows(columns, f, b):
    low = iota((columns.shape[0], 128), 1) < HEAD_DIM
    return jnp.where(low, columns[:, f : f + 1], columns[:, b : b + 1])


def conv_silu(own, other, before, after, taps, first):
    own, other = own.astype(F32), other.astype(F32)
    x = jnp.concatenate(
        [jnp.where(first, own, other), jnp.where(first, other, own)], axis=0
    )
    rows = x.shape[0]
    row = iota(x.shape, 0)
    m1 = jnp.where(row == 0, before[1:2], pltpu.roll(x, 1, 0))
    m2 = jnp.where(
        row == 0, before[0:1], jnp.where(row == 1, before[1:2], pltpu.roll(x, 2, 0))
    )
    p1 = jnp.where(row == rows - 1, after[0:1], pltpu.roll(x, rows - 1, 0))
    total = m2 * taps[0:1] + m1 * taps[1:2] + x * taps[2:3] + p1 * taps[3:4]
    return (total / (1.0 + jnp.exp(-total))).astype(BF16)


def three(v):
    hi = v.astype(BF16)
    left = v - hi.astype(F32)
    mid = left.astype(BF16)
    return hi, mid, (left - mid.astype(F32)).astype(BF16)


def kernel(
    sizes,
    x_ref, b_ref, c_ref, z_ref, ra_ref, rr_ref, rf_ref,
    wx_ref, wb_ref, wc_ref, off_ref, spd_ref, gain_ref,
    out_ref,
    xo, bo, co, ro, hs, hr, ws, wr,
    cum_t, rate_t, fac_t, ecum_t,
    xc, bc, cc, yl, zs, gs,
    ts, tr, ls, lr, pre, pcl,
    ss, sl, yr, ylr, ypre, ypcl,
    zq, zql, zr, zlr,
    isd, ir, es, er,
    ys, yx,
    d_s, d_r, h_s, h_r, w_s, w_r,
    t_s, t_r, l_s, l_r, s_s, s_r, sl_s, sl_r,
    q_s, q_r, ql_s, ql_r, i_s, i_r, e_s, e_r, y_s, y_r,
):
    nx, ny, nz = sizes
    pairs = nx // 2
    xw, bw = pairs * PW, pairs * 2 * STATE
    x, c, z, y = (lax.axis_index(n) for n in ("x", "c", "z", "y"))
    first = c == 0
    partner = {"c": 1 - c}
    lin = (z * ny + y) * nx + x
    total_chips = nx * ny * nz
    has_prev, has_next = lin > 0, lin < total_chips - 1

    def chip(at):
        at = lax.rem(at + total_chips, total_chips)
        rest = at // nx
        return {"x": lax.rem(at, nx), "y": lax.rem(rest, ny), "z": rest // ny}

    target_exists = jnp.logical_or(
        jnp.logical_and(first, has_prev), jnp.logical_and(jnp.logical_not(first), has_next)
    )
    target = chip(jnp.where(first, lin - 1, lin + 1))

    barrier = pltpu.get_barrier_semaphore()

    def greet(device):
        pl.semaphore_signal(barrier, inc=1, device_id=device, device_id_type=MESH)

    greet(partner)

    @pl.loop(1, nx)
    def _(k):
        at = lax.rem(x + k, nx)
        greet({"x": at})
        greet({"x": at, "c": 1 - c})

    @pl.loop(1, ny)
    def _(k):
        greet({"y": lax.rem(y + k, ny)})

    @pl.loop(1, nz)
    def _(k):
        greet({"z": lax.rem(z + k, nz)})

    @pl.when(has_prev)
    def _():
        greet({**chip(lin - 1), "c": 1})

    @pl.when(has_next)
    def _():
        greet({**chip(lin + 1), "c": 0})

    group = 2 * x + c
    slot = lax.rem(group, nx)
    parity = lax.rem(slot, 2)
    place = (iota((GW, PW), 1) == iota((GW, PW), 0) + GW * parity).astype(BF16)
    ws[:, 0:PW] = mm(wx_ref[...], place).astype(BF16)
    ws[:, PW : PW + STATE] = wb_ref[...]
    ws[:, PW + STATE : PW + 2 * STATE] = wc_ref[...]
    lane = iota((1, 128), 1)
    base = 16 * (slot // 2) + HPG * parity
    tap = iota((TAPS, 128), 0)
    for k, ref in enumerate((off_ref, spd_ref)):
        row = jnp.zeros((1, 128), F32)
        for d in range(2):
            for i in range(HPG):
                row = jnp.where(lane == base + 8 * d + i, ref[d : d + 1, i : i + 1], row)
        parts = [v.astype(F32) for v in three(row)]
        rows = jnp.where(
            tap == 0, parts[0], jnp.where(tap == 1, parts[1], jnp.where(tap == 2, parts[2], 0.0))
        )
        lo = PW + (2 + k) * STATE
        ws[:, lo : lo + STATE] = rows.astype(BF16)

    at = 0
    for ref, width in ((x_ref, xw), (b_ref, bw), (c_ref, bw)):
        for half in range(2):
            cols = pl.ds(half * width, width)
            last = ref[0, TOK - 16 : TOK, cols].astype(F32)[8:16]
            start = ref[0, 0:16, cols].astype(F32)[0:8]
            rows = jnp.where(first, start, pltpu.roll(last, 2, 0))
            hs[half, :, at : at + width] = rows[0:2]
        at += width

    @pl.when(jnp.logical_not(has_prev))
    def _():
        hr[0] = jnp.zeros(hr.shape[1:], F32)

    @pl.when(jnp.logical_not(has_next))
    def _():
        hr[1] = jnp.zeros(hr.shape[1:], F32)

    expected = 1 + 2 * (nx - 1) + (ny - 1) + (nz - 1)
    pl.semaphore_wait(barrier, expected + jnp.where(target_exists, 2, 0))

    def half_of(ref, width, half):
        return ref.at[0, :, pl.ds(pl.multiple_of(half * width, 128), width)]

    rate_copies = [
        rcopy(ref.at[0], ro.at[k], d_s.at[k], d_r.at[k], partner)
        for k, ref in enumerate((ra_ref, rr_ref, rf_ref))
    ]
    data_copies = [
        rcopy(half_of(ref, width, 1 - c), dst, d_s.at[3 + k], d_r.at[3 + k], partner)
        for k, (ref, width, dst) in enumerate(((x_ref, xw, xo), (b_ref, bw, bo), (c_ref, bw, co)))
    ]

    to_core = group // nx

    def weight_copy(j):
        return rcopy(ws, wr.at[slot], w_s.at[j], w_r.at[slot], {"x": j, "c": to_core})

    def weight_is_mine(j):
        return jnp.logical_and(j == x, to_core == c)

    @pl.loop(0, nx)
    def _(k):
        j = lax.rem(x + nx // 2 + k, nx)

        @pl.when(jnp.logical_not(weight_is_mine(j)))
        def _():
            weight_copy(j).start()

    @pl.when(to_core == c)
    def _():
        wr[slot] = ws[...]

    for copy in rate_copies:
        copy.start()

    def halo_copy(half):
        return rcopy(
            hs.at[half], hr.at[1 - c], h_s.at[half], h_r.at[1 - c], {**target, "c": half}
        )

    @pl.when(target_exists)
    def _():
        for half in range(2):
            halo_copy(half).start()

    for copy in data_copies:
        copy.start()

    for copy in rate_copies:
        copy.wait_recv()

    n = 2 * TOK
    heads = ra_ref.shape[1]
    lanes, head = iota((128, heads), 0), iota((128, heads), 1)
    pair, rest = lanes // 16, lax.rem(lanes, 16)
    inside = lax.rem(rest, 8)
    valid = jnp.logical_and(inside < 6, pair < pairs)
    valid = jnp.logical_and(valid, head == 6 * pairs * c + 6 * pair + inside)
    pick_f = jnp.logical_and(valid, rest < 8).astype(F32)
    pick_b = jnp.logical_and(valid, rest >= 8).astype(F32)

    def both(ref, k):
        own, other = ref[0], ro[k]
        return jnp.concatenate(
            [jnp.where(first, own, other), jnp.where(first, other, own)], axis=1
        )

    raw = mm(pick_f, both(ra_ref, 0), HIGH) + mm(pick_b, both(rr_ref, 1), HIGH)
    fading = mm(pick_f + pick_b, both(rf_ref, 2), HIGH)

    @pl.loop(0, nx)
    def _(j):
        @pl.when(jnp.logical_not(nx * c + j == group))
        def _():
            rcopy(ws, wr.at[j], w_s.at[j], w_r.at[j], partner).wait_recv()

    def summed(lo):
        row = jnp.zeros((1, 128), F32)
        for j in range(nx):
            v = wr[j, :, lo : lo + 128].astype(F32)
            row = row + ((v[0:1] + v[1:2]) + v[2:3])
        return jnp.broadcast_to(row, (8, 128)).T[:, 0:1]

    offset, speed = summed(PW + 2 * STATE), summed(PW + 3 * STATE)
    pre_rate = raw + offset
    rate = jnp.maximum(pre_rate, 0.0) + jnp.log1p(jnp.exp(-jnp.abs(pre_rate)))
    log = fading - jnp.exp(speed) * rate
    row_i, col_i = iota((n, n), 0), iota((n, n), 1)
    forward = lax.rem(iota((128, 1), 0), 16) < 8
    upper, lower = (row_i <= col_i).astype(BF16), (row_i >= col_i).astype(BF16)
    parts = three(log)
    cum = jnp.where(
        forward,
        (mm(parts[2], upper) + mm(parts[1], upper)) + mm(parts[0], upper),
        (mm(parts[2], lower) + mm(parts[1], lower)) + mm(parts[0], lower),
    )
    span = jnp.where(forward, cum[:, n - 1 : n], cum[:, 0:1])
    cum_t[...] = cum
    rate_t[...] = rate
    fac_t[...] = rate * jnp.exp(span - cum)
    ecum_t[...] = jnp.exp(cum)

    @pl.when(has_prev)
    def _():
        rcopy(hs.at[0], hr.at[0], h_s.at[0], h_r.at[0], partner).wait_recv()

    @pl.when(has_next)
    def _():
        rcopy(hs.at[0], hr.at[1], h_s.at[0], h_r.at[1], partner).wait_recv()

    for copy in data_copies:
        copy.wait_recv()

    low = iota((1, 128), 1) < HEAD_DIM

    def rows_of(p):
        return pl.ds(pl.multiple_of(16 * p, 16), 16)

    def x_cols(p):
        return pl.ds(pl.multiple_of(PW * p, 128), PW)

    def b_cols(p):
        return pl.ds(pl.multiple_of(2 * STATE * p, 128), 2 * STATE)

    def state_copy(m, j):
        return rcopy(
            ts.at[m, j], tr.at[m, x], t_s.at[m * nx + j], t_r.at[m * nx + x], {"x": j}
        )

    def log_copy(j):
        return rcopy(ls.at[j], lr.at[x], l_s.at[j], l_r.at[x], {"x": j})

    def state_conv(p, own, other, at, lo):
        start = pl.multiple_of(2 * STATE * p, 128)
        taps = jnp.concatenate(
            [wr[2 * p, :, lo : lo + STATE], wr[2 * p + 1, :, lo : lo + STATE]], axis=1
        ).astype(F32)
        cols_in = pl.ds(pl.multiple_of(c * bw + start, 128), 2 * STATE)
        cols_h = pl.ds(pl.multiple_of(at + start, 128), 2 * STATE)
        return conv_silu(
            own[0, :, cols_in], other[:, b_cols(p)], hr[0, :, cols_h], hr[1, :, cols_h],
            taps, first,
        )

    @pl.loop(0, pairs)
    def _(k):
        p = lax.rem(x // 2 + 1 + k, pairs)
        w0, w1 = wr[2 * p].astype(F32), wr[2 * p + 1].astype(F32)
        cols, start = x_cols(p), pl.multiple_of(PW * p, 128)
        x_cols_in = pl.ds(pl.multiple_of(c * xw + start, 128), PW)
        xv = conv_silu(
            x_ref[0, :, x_cols_in], xo[:, cols], hr[0, :, cols], hr[1, :, cols],
            w0[:, 0:PW] + w1[:, 0:PW], first,
        )
        xc[:, cols] = xv
        bv = state_conv(p, b_ref, bo, xw, PW)
        bc[:, b_cols(p)] = bv
        factors = fac_t[rows_of(p)].T
        cums = cum_t[rows_of(p)].T
        direction = iota((1, 16), 1) < 8
        spans = jnp.where(direction, cums[n - 1 : n], cums[0:1])
        xf = xv.astype(F32)
        bf = bv.astype(F32)
        for q in range(2):
            j = 2 * p + q
            scaled, span_row = [], []
            for i in range(HPG):
                f, g = HPG * q + i, 8 + HPG * q + i
                v = xf[:, 128 * (f // 2) : 128 * (f // 2 + 1)]
                turned = pltpu.roll(v, HEAD_DIM, 1)
                twice = jnp.where(low, v, turned) if f % 2 == 0 else jnp.where(low, turned, v)
                scaled.append(twice * head_rows(factors, f, g))
                span_row.append(head_rows(spans, f, g))
            scaled = jnp.concatenate(scaled, axis=1)
            span_row = jnp.concatenate(span_row, axis=1)
            hi = scaled.astype(BF16)
            lo = (scaled - hi.astype(F32)).astype(BF16)
            bt = bf[:, q * STATE : (q + 1) * STATE].T.astype(BF16)
            update = (mm(bt, hi) + mm(bt, lo)).astype(BF16)

            @pl.when(j == x)
            def _():
                for m in range(HPG):
                    tr[m, x] = update[:, 128 * m : 128 * (m + 1)]
                lr[x] = span_row

            @pl.when(j != x)
            def _():
                ls[j] = span_row
                for m in range(HPG):
                    ts[m, j] = update[:, 128 * m : 128 * (m + 1)]
                log_copy(j).start()
                state_copy(0, j).start()

    for m in range(1, HPG):
        @pl.loop(1, nx)
        def _(k):
            state_copy(m, lax.rem(x + k, nx)).start()

    @pl.loop(0, pairs)
    def _(p):
        cum_r, rate_r = cum_t[rows_of(p)], rate_t[rows_of(p)]
        cum_c = cum_r.T
        cv = state_conv(p, c_ref, co, xw + bw, PW + STATE)
        cc[:, b_cols(p)] = cv
        xv, bv = xc[:, x_cols(p)], bc[:, b_cols(p)]
        below, above = col_i < row_i, col_i > row_i
        products = []
        for q in range(2):
            scores = lax.dot_general(
                cv[:, q * STATE : (q + 1) * STATE], bv[:, q * STATE : (q + 1) * STATE],
                (((1,), (1,)), ((), ())), preferred_element_type=F32,
            )
            for i in range(HPG):
                f, g = HPG * q + i, 8 + HPG * q + i
                gap = jnp.where(
                    above,
                    cum_c[:, g : g + 1] - cum_r[g : g + 1],
                    cum_c[:, f : f + 1] - cum_r[f : f + 1],
                )
                r_f, r_b = rate_r[f : f + 1], rate_r[g : g + 1]
                coef = jnp.where(below, r_f, jnp.where(above, r_b, r_f + r_b))
                weights = (scores * jnp.exp(gap) * coef).astype(BF16)
                v = f // 2
                products.append(mm(weights, xv[:, 128 * v : 128 * (v + 1)]))
        yl[:, x_cols(p)] = jnp.concatenate(
            [jnp.where(low, products[2 * v], products[2 * v + 1]) for v in range(HPG)], axis=1
        )

    def gate_cols(k):
        return pl.ds(pl.multiple_of(k * PW, 128), PW)

    ry = STATE // ny

    def y_rows(j):
        return pl.ds(pl.multiple_of(ry * j, ry), ry)

    def part(row, m):
        return row[:, 128 * m : 128 * (m + 1)]

    def along_x(m):
        @pl.loop(0, nx)
        def _(k):
            @pl.when(k != x)
            def _():
                if m == 0:
                    rcopy(ls.at[k], lr.at[k], l_s.at[k], l_r.at[k], partner).wait_recv()
                at = m * nx + k
                rcopy(ts.at[m, k], tr.at[m, k], t_s.at[at], t_r.at[at], partner).wait_recv()

        if m == 0:
            pcl[0] = jnp.zeros(pcl.shape[1:], F32)
            wide = jnp.concatenate([low] * HPG, axis=1)

            @pl.loop(0, nx)
            def _(k):
                pcl[k + 1] = pcl[k] + jnp.where(wide, lr[k], lr[nx - 1 - k])

            sl[...] = pcl[nx]

        pre[m, 0] = jnp.zeros(pre.shape[2:], F32)

        @pl.loop(0, nx)
        def _(k):
            d = jnp.where(low, part(lr[k], m), part(lr[nx - 1 - k], m))
            v = jnp.where(low, tr[m, k].astype(F32), tr[m, nx - 1 - k].astype(F32))
            pre[m, k + 1] = pre[m, k] * jnp.exp(d) + v

        ss[m] = pre[m, nx].astype(ss.dtype)

        @pl.loop(1, ny)
        def _(k):
            j = lax.rem(y + k, ny)
            if m == 0:
                rcopy(sl, ylr.at[y], sl_s.at[j], sl_r.at[y], {"y": j}).start()
            total_copy(m, j).start()

        yr[m, y] = ss[m, y_rows(y)]
        if m == 0:
            ylr[y] = sl[...]

    def total_copy(m, j):
        return rcopy(
            ss.at[m, y_rows(j)], yr.at[m, y], s_s.at[m * ny + j], s_r.at[m * ny + y], {"y": j}
        )

    def plane_copy(m, j):
        return rcopy(zq.at[m], zr.at[m, z], q_s.at[m * nz + j], q_r.at[m * nz + z], {"z": j})

    def incoming_copy(m, j):
        return rcopy(
            isd.at[m, j], ir.at[m, y_rows(y)], i_s.at[m * ny + j], i_r.at[m * ny + y], {"y": j}
        )

    def entry_copy(m, j):
        return rcopy(
            es.at[m, j], er.at[m, x], e_s.at[m * nx + j], e_r.at[m * nx + x], {"x": j}
        )

    def along_y(m):
        @pl.loop(1, ny)
        def _(k):
            j = lax.rem(y + k, ny)
            if m == 0:
                rcopy(sl, ylr.at[j], sl_s.at[j], sl_r.at[j], {"y": j}).wait_recv()
            at = m * ny + j
            rcopy(ss.at[m, y_rows(j)], yr.at[m, j], s_s.at[at], s_r.at[at], {"y": j}).wait_recv()

        if m == 0:
            ypcl[0] = jnp.zeros(ypcl.shape[1:], F32)
            wide = jnp.concatenate([low] * HPG, axis=1)

            @pl.loop(0, ny)
            def _(k):
                ypcl[k + 1] = ypcl[k] + jnp.where(wide, ylr[k], ylr[ny - 1 - k])

            zql[...] = ypcl[ny]

        ypre[m, 0] = jnp.zeros(ypre.shape[2:], F32)

        @pl.loop(0, ny)
        def _(k):
            d = jnp.where(low, part(ylr[k], m), part(ylr[ny - 1 - k], m))
            v = jnp.where(low, yr[m, k].astype(F32), yr[m, ny - 1 - k].astype(F32))
            ypre[m, k + 1] = ypre[m, k] * jnp.exp(d) + v

        zq[m] = ypre[m, ny]

        @pl.loop(1, nz)
        def _(k):
            j = lax.rem(z + k, nz)
            if m == 0:
                rcopy(zql, zlr.at[z], ql_s.at[j], ql_r.at[z], {"z": j}).start()
            plane_copy(m, j).start()

        zr[m, z] = zq[m]
        if m == 0:
            zlr[z] = zql[...]

    def along_z(m):
        @pl.loop(1, nz)
        def _(k):
            j = lax.rem(z + k, nz)
            if m == 0:
                rcopy(zql, zlr.at[j], ql_s.at[j], ql_r.at[j], {"z": j}).wait_recv()
            at = m * nz + j
            rcopy(zq.at[m], zr.at[m, j], q_s.at[at], q_r.at[at], {"z": j}).wait_recv()

        running = jnp.zeros((ry, 128), F32)
        entering = jnp.zeros((ry, 128), F32)
        wanted = jnp.where(low, z, nz - 1 - z)
        for k in range(nz):
            entering = jnp.where(wanted == k, running, entering)
            d = jnp.where(low, part(zlr[k], m), part(zlr[nz - 1 - k], m))
            v = jnp.where(low, zr[m, k], zr[m, nz - 1 - k])
            running = running * jnp.exp(d) + v

        def incoming(j):
            f = ypre[m, j] + jnp.exp(part(ypcl[j], m)) * entering
            b = ypre[m, ny - 1 - j] + jnp.exp(part(ypcl[ny - 1 - j], m)) * entering
            return jnp.where(low, f, b).astype(ir.dtype)

        @pl.loop(1, ny)
        def _(k):
            j = lax.rem(y + k, ny)
            isd[m, j] = incoming(j)
            incoming_copy(m, j).start()

        ir[m, y_rows(y)] = incoming(y)

    def back_along_x(m):
        @pl.loop(1, ny)
        def _(k):
            j = lax.rem(y + k, ny)
            at = m * ny + j
            rcopy(isd.at[m, j], ir.at[m, y_rows(j)], i_s.at[at], i_r.at[at], {"y": j}).wait_recv()

        def entry(j):
            here = ir[m].astype(F32)
            f = pre[m, j] + jnp.exp(part(pcl[j], m)) * here
            b = pre[m, nx - 1 - j] + jnp.exp(part(pcl[nx - 1 - j], m)) * here
            return jnp.where(low, f, b).astype(BF16)

        @pl.loop(1, nx)
        def _(k):
            j = lax.rem(x + k, nx)
            es[m, j] = entry(j)
            entry_copy(m, j).start()

        er[m, x] = entry(x)

    def pair_at(k):
        away = (k + 1) // 2
        return lax.rem(x // 2 + jnp.where(lax.rem(k, 2) == 1, away, pairs - away), pairs)

    def carried(m, p):
        cv = cc[:, b_cols(p)]
        decays = ecum_t[rows_of(p)].T
        for q in range(2):
            j = 2 * p + q
            f, g = HPG * q + m, 8 + HPG * q + m

            @pl.when(j != x)
            def _():
                at = m * nx + j
                rcopy(es.at[m, j], er.at[m, j], e_s.at[at], e_r.at[at], partner).wait_recv()

            v = mm(part(cv, q), er[m, j]) * head_rows(decays, f, g)
            v = v + pltpu.roll(v, HEAD_DIM, 1)
            mine = low if f % 2 == 0 else jnp.logical_not(low)
            cols = pl.ds(pl.multiple_of(PW * p + 128 * (f // 2), 128), 128)
            yl[:, cols] = yl[:, cols] + jnp.where(mine, v, 0.0)

    along_x(0)

    for k in range(2 * xw // 128):
        cols = slice(128 * k, 128 * (k + 1))
        gs[:, cols] = gain_ref[cols].astype(F32).reshape(1, 128)

    @pl.loop(0, 2 * pairs)
    def _(k):
        zz = z_ref[0, :, gate_cols(k)].astype(F32)
        zs[:, gate_cols(k)] = zz / (1.0 + jnp.exp(-zz))

    along_x(1)
    along_y(0)
    along_x(2)
    along_z(0)
    along_y(1)
    back_along_x(0)
    along_y(2)
    along_z(1)
    back_along_x(1)
    along_z(2)

    for copy in rate_copies + data_copies:
        copy.wait_send()

    @pl.when(target_exists)
    def _():
        for half in range(2):
            halo_copy(half).wait_send()

    @pl.loop(0, nx)
    def _(j):
        @pl.when(jnp.logical_not(weight_is_mine(j)))
        def _():
            weight_copy(j).wait_send()

        @pl.when(j != x)
        def _():
            log_copy(j).wait_send()
            for m in range(HPG):
                state_copy(m, j).wait_send()

    @pl.loop(1, ny)
    def _(k):
        j = lax.rem(y + k, ny)
        rcopy(sl, ylr.at[y], sl_s.at[j], sl_r.at[y], {"y": j}).wait_send()
        for m in range(HPG):
            total_copy(m, j).wait_send()

    @pl.loop(1, nz)
    def _(k):
        j = lax.rem(z + k, nz)
        rcopy(zql, zlr.at[z], ql_s.at[j], ql_r.at[z], {"z": j}).wait_send()
        for m in range(HPG):
            plane_copy(m, j).wait_send()

    back_along_x(2)

    @pl.loop(1, ny)
    def _(k):
        for m in range(HPG):
            incoming_copy(m, lax.rem(y + k, ny)).wait_send()

    for m in range(HPG - 1):
        @pl.loop(0, pairs)
        def _(k):
            carried(m, pair_at(k))

    @pl.loop(1, nx)
    def _(k):
        for m in range(HPG - 1):
            entry_copy(m, lax.rem(x + k, nx)).wait_send()

    block_r, block_c = iota((128, 128), 0) // HEAD_DIM, iota((128, 128), 1) // HEAD_DIM
    ones = (block_r == block_c).astype(BF16)

    def gate(mixed, cols):
        g = mixed.astype(F32) * zs[:, cols]
        sq = g * g
        hi = sq.astype(BF16)
        lo = (sq - hi.astype(F32)).astype(BF16)
        means = jnp.concatenate(
            [mm(part(hi, v), ones) + mm(part(lo, v), ones) for v in range(HPG)], axis=1
        ) * (1.0 / HEAD_DIM)
        normed = g * lax.rsqrt(means + 1e-06)
        out_ref[0, :, cols] = (normed * gs[:, cols]).astype(BF16)

    def own_cols(p, half):
        return pl.ds(pl.multiple_of(half * xw + PW * p, 128), PW)

    def mixed_copy(p):
        return rcopy(ys.at[p], yx.at[p], y_s.at[p], y_r.at[p], partner)

    def other_half(p):
        mixed_copy(p).wait_recv()
        gate(yx[p], own_cols(p, 1 - c))

    @pl.loop(0, pairs)
    def _(k):
        p = pair_at(k)
        carried(HPG - 1, p)
        mixed = yl[:, x_cols(p)]
        top, bottom = mixed[0:TOK].astype(BF16), mixed[TOK:n].astype(BF16)
        ys[p] = jnp.where(first, bottom, top)
        mixed_copy(p).start()
        gate(jnp.where(first, top, bottom), own_cols(p, c))

        @pl.when(k > 0)
        def _():
            other_half(pair_at(k - 1))

    other_half(pair_at(pairs - 1))

    @pl.loop(1, nx)
    def _(k):
        entry_copy(HPG - 1, lax.rem(x + k, nx)).wait_send()

    @pl.loop(0, pairs)
    def _(p):
        mixed_copy(p).wait_send()


def local(sizes, *args):
    nx, ny, nz = sizes
    pairs = nx // 2
    xw, bw = pairs * PW, pairs * 2 * STATE
    n = 2 * TOK
    ry = STATE // ny
    args = list(args)
    args[4:7] = [jnp.swapaxes(a, 1, 2) for a in args[4:7]]
    dma = pltpu.SemaphoreType.DMA
    vmem = pltpu.VMEM
    wide = PW + 4 * STATE
    scratch = [
        vmem((TOK, xw), BF16), vmem((TOK, bw), BF16), vmem((TOK, bw), BF16),
        vmem((3, args[4].shape[1], TOK), F32),
        vmem((2, 2, xw + 2 * bw), F32), vmem((2, 2, xw + 2 * bw), F32),
        vmem((TAPS, wide), BF16), vmem((nx, TAPS, wide), BF16),
        vmem((128, n), F32), vmem((128, n), F32), vmem((128, n), F32), vmem((128, n), F32),
        vmem((n, xw), BF16), vmem((n, bw), BF16), vmem((n, bw), BF16), vmem((n, xw), F32),
        vmem((TOK, 2 * xw), F32), vmem((1, 2 * xw), F32),
        vmem((HPG, nx, STATE, 128), BF16), vmem((HPG, nx, STATE, 128), BF16),
        vmem((nx, 1, PW), F32), vmem((nx, 1, PW), F32),
        vmem((HPG, nx + 1, STATE, 128), F32), vmem((nx + 1, 1, PW), F32),
        vmem((HPG, STATE, 128), BF16), vmem((1, PW), F32),
        vmem((HPG, ny, ry, 128), BF16), vmem((ny, 1, PW), F32),
        vmem((HPG, ny + 1, ry, 128), F32), vmem((ny + 1, 1, PW), F32),
        vmem((HPG, ry, 128), F32), vmem((1, PW), F32),
        vmem((HPG, nz, ry, 128), F32), vmem((nz, 1, PW), F32),
        vmem((HPG, ny, ry, 128), BF16), vmem((HPG, STATE, 128), BF16),
        vmem((HPG, nx, STATE, 128), BF16), vmem((HPG, nx, STATE, 128), BF16),
        vmem((pairs, TOK, PW), BF16), vmem((pairs, TOK, PW), BF16),
    ]
    hx, hy, hz = HPG * nx, HPG * ny, HPG * nz
    counts = [6, 6, 2, 2, nx, nx, hx, hx, nx, nx, hy, hy, ny, ny, hz, hz, nz, nz, hy, hy, hx, hx, pairs, pairs]
    scratch += [dma((k,)) for k in counts]
    return pl.pallas_call(
        functools.partial(kernel, sizes),
        out_shape=jax.ShapeDtypeStruct(args[0].shape, BF16),
        in_specs=[pl.BlockSpec(memory_space=pltpu.VMEM)] * len(args),
        out_specs=pl.BlockSpec(memory_space=pltpu.VMEM),
        scratch_shapes=scratch,
        compiler_params=pltpu.CompilerParams(
            collective_id=0, has_side_effects=True, vmem_limit_bytes=60 * 1024 * 1024
        ),
        name="mixer",
    )(*args)


def solution(mesh):
    sp, dp = mesh.shape["sp"], mesh.shape["dp"]
    nx = sp // 2
    ny = max(k for k in range(1, dp + 1) if dp % k == 0 and k * k <= dp)
    nz = dp // ny
    torus = Mesh(mesh.devices.reshape(nx, 2, nz, ny), ("x", "c", "z", "y"))
    rows = P(("z", "y"), ("x", "c"), None)
    cols = P(None, ("x", "c"))
    return jax.shard_map(
        functools.partial(local, (nx, ny, nz)),
        mesh=torus,
        in_specs=(rows,) * 7 + (cols,) * 5 + (P(),),
        out_specs=rows,
        check_vma=False,
    )
```

```python
import functools

import jax
import jax.numpy as jnp
from jax import lax
from jax.experimental import pallas as pl
from jax.experimental.pallas import tpu as pltpu
from jax.sharding import Mesh
from jax.sharding import PartitionSpec as P

MESH = pl.DeviceIdType.MESH
HEAD_DIM = 64
STATE = 128
TOK = 128
HPG = 3
TAPS = 4
GW = HPG * HEAD_DIM
PW = 2 * GW
HIGH = lax.Precision.HIGHEST
F32 = jnp.float32
BF16 = jnp.bfloat16


def iota(shape, dim):
    return lax.broadcasted_iota(jnp.int32, shape, dim)


def mm(a, b, precision=None):
    return jnp.dot(a, b, preferred_element_type=F32, precision=precision)


def rcopy(src, dst, send_sem, recv_sem, device):
    return pltpu.make_async_remote_copy(
        src_ref=src,
        dst_ref=dst,
        send_sem=send_sem,
        recv_sem=recv_sem,
        device_id=device,
        device_id_type=MESH,
    )


def head_rows(columns, f, b):
    low = iota((columns.shape[0], 128), 1) < HEAD_DIM
    return jnp.where(low, columns[:, f : f + 1], columns[:, b : b + 1])


def silu(t):
    h = 0.5 * t
    return h + h * jnp.tanh(h)


def conv_silu(own, other, before, after, taps, first):
    top, bottom = jnp.where(first, own, other), jnp.where(first, other, own)
    edge = iota((8, own.shape[1]), 0)
    ahead = jnp.where(edge == 6, before[0:1], jnp.where(edge == 7, before[1:2], 0.0))
    behind = jnp.where(edge == 0, after[0:1], 0.0)
    x = jnp.concatenate([ahead, top.astype(F32), bottom.astype(F32), behind], axis=0)
    rows = x.shape[0]
    inner = slice(8, rows - 8)
    m2, m1, p1 = (pltpu.roll(x, k, 0)[inner] for k in (2, 1, rows - 1))
    total = m2 * taps[0:1] + m1 * taps[1:2] + x[inner] * taps[2:3] + p1 * taps[3:4]
    return silu(total).astype(BF16)


def three(v):
    hi = v.astype(BF16)
    left = v - hi.astype(F32)
    mid = left.astype(BF16)
    return hi, mid, (left - mid.astype(F32)).astype(BF16)


def kernel(
    sizes,
    x_in, b_in, c_in, z_in, ra_in, rr_in, rf_in,
    wx_in, wb_in, wc_in, off_in, spd_in, gain_in,
    out_ref,
    x_ref, b_ref, c_ref, z_ref, ra_ref, rr_ref, rf_ref,
    wx_ref, wb_ref, wc_ref, off_ref, spd_ref, gain_ref, in_s,
    xo, bo, co, ro, hs, hr, ws, wr,
    cum_t, rate_t, fac_t, ecum_t, span_row_of,
    xc, bc, cc, yl, zs, gs,
    ts, tr, ls, lr, pre, pcl,
    ss, sl, yr, ylr, ypre, ypcl,
    zq, zql, zr, zlr,
    isd, ir, es, er,
    ys, yx,
    d_s, d_r, h_s, h_r, w_s, w_r,
    t_s, t_r, l_s, l_r, s_s, s_r, sl_s, sl_r,
    q_s, q_r, ql_s, ql_r, i_s, i_r, e_s, e_r, y_s, y_r,
):
    sources = (
        wx_in, wb_in, wc_in, off_in, spd_in, x_in, b_in, c_in, ra_in, rr_in, rf_in, z_in, gain_in
    )
    places = (
        wx_ref, wb_ref, wc_ref, off_ref, spd_ref, x_ref, b_ref, c_ref, ra_ref, rr_ref, rf_ref,
        z_ref, gain_ref,
    )
    loads = [
        pltpu.make_async_copy(source, place, in_s.at[k])
        for k, (source, place) in enumerate(zip(sources, places))
    ]
    for load in loads:
        load.start()

    nx, ny, nz = sizes
    pairs = nx // 2
    xw, bw = pairs * PW, pairs * 2 * STATE
    x, c, z, y = (lax.axis_index(n) for n in ("x", "c", "z", "y"))
    first = c == 0
    partner = {"c": 1 - c}
    lin = (z * ny + y) * nx + x
    total_chips = nx * ny * nz
    has_prev, has_next = lin > 0, lin < total_chips - 1

    def chip(at):
        at = lax.rem(at + total_chips, total_chips)
        rest = at // nx
        return {"x": lax.rem(at, nx), "y": lax.rem(rest, ny), "z": rest // ny}

    target_exists = jnp.logical_or(
        jnp.logical_and(first, has_prev), jnp.logical_and(jnp.logical_not(first), has_next)
    )
    target = chip(jnp.where(first, lin - 1, lin + 1))

    barrier = pltpu.get_barrier_semaphore()

    def greet(device):
        pl.semaphore_signal(barrier, inc=1, device_id=device, device_id_type=MESH)

    greet(partner)

    @pl.loop(1, nx)
    def _(k):
        at = lax.rem(x + k, nx)
        greet({"x": at})
        greet({"x": at, "c": 1 - c})

    @pl.loop(1, ny)
    def _(k):
        greet({"y": lax.rem(y + k, ny)})

    @pl.loop(1, nz)
    def _(k):
        greet({"z": lax.rem(z + k, nz)})

    @pl.when(has_prev)
    def _():
        greet({**chip(lin - 1), "c": 1})

    @pl.when(has_next)
    def _():
        greet({**chip(lin + 1), "c": 0})

    for load in loads[:5]:
        load.wait()

    group = 2 * x + c
    slot = lax.rem(group, nx)
    parity = lax.rem(slot, 2)
    place = (iota((GW, PW), 1) == iota((GW, PW), 0) + GW * parity).astype(BF16)
    ws[:, 0:PW] = mm(wx_ref[...], place).astype(BF16)
    ws[:, PW : PW + STATE] = wb_ref[...]
    ws[:, PW + STATE : PW + 2 * STATE] = wc_ref[...]
    lane = iota((1, 128), 1)
    base = 16 * (slot // 2) + HPG * parity
    tap = iota((TAPS, 128), 0)
    for k, ref in enumerate((off_ref, spd_ref)):
        row = jnp.zeros((1, 128), F32)
        for d in range(2):
            for i in range(HPG):
                row = jnp.where(lane == base + 8 * d + i, ref[d : d + 1, i : i + 1], row)
        parts = [v.astype(F32) for v in three(row)]
        rows = jnp.where(
            tap == 0, parts[0], jnp.where(tap == 1, parts[1], jnp.where(tap == 2, parts[2], 0.0))
        )
        lo = PW + (2 + k) * STATE
        ws[:, lo : lo + STATE] = rows.astype(BF16)

    for load in loads[5:8]:
        load.wait()

    at = 0
    for ref, width in ((x_ref, xw), (b_ref, bw), (c_ref, bw)):
        for half in range(2):
            cols = pl.ds(half * width, width)
            last = ref[0, TOK - 16 : TOK, cols].astype(F32)[8:16]
            start = ref[0, 0:16, cols].astype(F32)[0:8]
            rows = jnp.where(first, start, pltpu.roll(last, 2, 0))
            hs[half, :, at : at + width] = rows[0:2]
        at += width

    @pl.when(jnp.logical_not(has_prev))
    def _():
        hr[0] = jnp.zeros(hr.shape[1:], F32)

    @pl.when(jnp.logical_not(has_next))
    def _():
        hr[1] = jnp.zeros(hr.shape[1:], F32)

    for load in loads[8:]:
        load.wait()

    expected = 1 + 2 * (nx - 1) + (ny - 1) + (nz - 1)
    pl.semaphore_wait(barrier, expected + jnp.where(target_exists, 2, 0))

    def half_of(ref, width, half):
        return ref.at[0, :, pl.ds(pl.multiple_of(half * width, 128), width)]

    rate_copies = [
        rcopy(ref.at[0], ro.at[k], d_s.at[k], d_r.at[k], partner)
        for k, ref in enumerate((ra_ref, rr_ref, rf_ref))
    ]
    data_copies = [
        rcopy(half_of(ref, width, 1 - c), dst, d_s.at[3 + k], d_r.at[3 + k], partner)
        for k, (ref, width, dst) in enumerate(((x_ref, xw, xo), (b_ref, bw, bo), (c_ref, bw, co)))
    ]

    to_core = group // nx

    def weight_copy(j):
        return rcopy(ws, wr.at[slot], w_s.at[j], w_r.at[slot], {"x": j, "c": to_core})

    def weight_is_mine(j):
        return jnp.logical_and(j == x, to_core == c)

    @pl.loop(0, nx)
    def _(k):
        j = lax.rem(x + nx // 2 + k, nx)

        @pl.when(jnp.logical_not(weight_is_mine(j)))
        def _():
            weight_copy(j).start()

    @pl.when(to_core == c)
    def _():
        wr[slot] = ws[...]

    for copy in rate_copies:
        copy.start()

    def halo_copy(half):
        return rcopy(
            hs.at[half], hr.at[1 - c], h_s.at[half], h_r.at[1 - c], {**target, "c": half}
        )

    @pl.when(target_exists)
    def _():
        for half in range(2):
            halo_copy(half).start()

    for copy in data_copies:
        copy.start()

    for copy in rate_copies:
        copy.wait_recv()

    n = 2 * TOK
    heads = ra_ref.shape[1]
    lanes, head = iota((128, heads), 0), iota((128, heads), 1)
    pair, rest = lanes // 16, lax.rem(lanes, 16)
    inside = lax.rem(rest, 8)
    valid = jnp.logical_and(inside < 6, pair < pairs)
    valid = jnp.logical_and(valid, head == 6 * pairs * c + 6 * pair + inside)
    pick_f = jnp.logical_and(valid, rest < 8).astype(F32)
    pick_b = jnp.logical_and(valid, rest >= 8).astype(F32)

    def both(ref, k):
        own, other = ref[0], ro[k]
        return jnp.concatenate(
            [jnp.where(first, own, other), jnp.where(first, other, own)], axis=1
        )

    raw = mm(pick_f, both(ra_ref, 0), HIGH) + mm(pick_b, both(rr_ref, 1), HIGH)
    fading = mm(pick_f + pick_b, both(rf_ref, 2), HIGH)

    def gate_cols(k):
        return pl.ds(pl.multiple_of(k * PW, 128), PW)

    for k in range(2 * xw // 128):
        cols = slice(128 * k, 128 * (k + 1))
        gs[:, cols] = gain_ref[cols].astype(F32).reshape(1, 128)

    @pl.loop(0, 2 * pairs)
    def _(k):
        zz = z_ref[0, :, gate_cols(k)].astype(F32)
        zs[:, gate_cols(k)] = silu(zz)

    @pl.loop(0, nx)
    def _(j):
        @pl.when(jnp.logical_not(nx * c + j == group))
        def _():
            rcopy(ws, wr.at[j], w_s.at[j], w_r.at[j], partner).wait_recv()

    def summed(lo):
        row = jnp.zeros((1, 128), F32)
        for j in range(nx):
            v = wr[j, :, lo : lo + 128].astype(F32)
            row = row + ((v[0:1] + v[1:2]) + v[2:3])
        return jnp.broadcast_to(row, (8, 128)).T[:, 0:1]

    offset, speed = summed(PW + 2 * STATE), summed(PW + 3 * STATE)
    pre_rate = raw + offset
    rate = jnp.maximum(pre_rate, 0.0) + jnp.log1p(jnp.exp(-jnp.abs(pre_rate)))
    log = fading - jnp.exp(speed) * rate
    row_i, col_i = iota((n, n), 0), iota((n, n), 1)
    forward = lax.rem(iota((128, 1), 0), 16) < 8
    upper, lower = (row_i <= col_i).astype(BF16), (row_i >= col_i).astype(BF16)
    parts = three(log)
    cum = jnp.where(
        forward,
        (mm(parts[2], upper) + mm(parts[1], upper)) + mm(parts[0], upper),
        (mm(parts[2], lower) + mm(parts[1], lower)) + mm(parts[0], lower),
    )
    span = jnp.where(forward, cum[:, n - 1 : n], cum[:, 0:1])
    span_line = jnp.broadcast_to(span, (128, 128)).T[0:1]
    for p in range(pairs):
        span_row_of[p] = span_line[:, 16 * p : 16 * (p + 1)]
    cum_t[...] = cum
    rate_t[...] = rate
    fac_t[...] = rate * jnp.exp(span - cum)
    ecum_t[...] = jnp.exp(cum)

    @pl.when(has_prev)
    def _():
        rcopy(hs.at[0], hr.at[0], h_s.at[0], h_r.at[0], partner).wait_recv()

    @pl.when(has_next)
    def _():
        rcopy(hs.at[0], hr.at[1], h_s.at[0], h_r.at[1], partner).wait_recv()

    for copy in data_copies:
        copy.wait_recv()

    low = iota((1, 128), 1) < HEAD_DIM

    def rows_of(p):
        return pl.ds(pl.multiple_of(16 * p, 16), 16)

    def x_cols(p):
        return pl.ds(pl.multiple_of(PW * p, 128), PW)

    def b_cols(p):
        return pl.ds(pl.multiple_of(2 * STATE * p, 128), 2 * STATE)

    half_rows = STATE // 2
    chunks = 2 * HPG

    def rows_in(u):
        return pl.ds(half_rows * (u % 2), half_rows)

    def state_copy(u, j):
        return rcopy(
            ts.at[u // 2, j, rows_in(u)], tr.at[u // 2, x, rows_in(u)],
            t_s.at[u * nx + j], t_r.at[u * nx + x], {"x": j},
        )

    def send_state(u, p):
        for q in range(2):
            @pl.when(2 * p + q != x)
            def _():
                state_copy(u, 2 * p + q).start()

    def conv_pair(k):
        return lax.rem(x // 2 + 1 + k, pairs)

    def log_copy(j):
        return rcopy(ls.at[j], lr.at[x], l_s.at[j], l_r.at[x], {"x": j})

    def state_conv(p, own, other, at, lo):
        start = pl.multiple_of(2 * STATE * p, 128)
        taps = jnp.concatenate(
            [wr[2 * p, :, lo : lo + STATE], wr[2 * p + 1, :, lo : lo + STATE]], axis=1
        ).astype(F32)
        cols_in = pl.ds(pl.multiple_of(c * bw + start, 128), 2 * STATE)
        cols_h = pl.ds(pl.multiple_of(at + start, 128), 2 * STATE)
        return conv_silu(
            own[0, :, cols_in], other[:, b_cols(p)], hr[0, :, cols_h], hr[1, :, cols_h],
            taps, first,
        )

    @pl.loop(0, pairs)
    def _(k):
        p = conv_pair(k)
        w0, w1 = wr[2 * p].astype(F32), wr[2 * p + 1].astype(F32)
        cols, start = x_cols(p), pl.multiple_of(PW * p, 128)
        x_cols_in = pl.ds(pl.multiple_of(c * xw + start, 128), PW)
        xv = conv_silu(
            x_ref[0, :, x_cols_in], xo[:, cols], hr[0, :, cols], hr[1, :, cols],
            w0[:, 0:PW] + w1[:, 0:PW], first,
        )
        xc[:, cols] = xv
        bv = state_conv(p, b_ref, bo, xw, PW)
        bc[:, b_cols(p)] = bv
        factors, spans = fac_t[rows_of(p)], span_row_of[p]
        bf = bv.astype(F32)
        for q in range(2):
            j = 2 * p + q
            bt = bf[:, q * STATE : (q + 1) * STATE].T
            update, span_row = [], []
            for i in range(HPG):
                f, g = HPG * q + i, 8 + HPG * q + i
                v = xv[:, 128 * (f // 2) : 128 * (f // 2 + 1)]
                ahead = mm((bt * factors[f : f + 1]).astype(BF16), v)
                back = mm((bt * factors[g : g + 1]).astype(BF16), v)
                if f % 2 == 0:
                    both_ways = jnp.where(low, ahead, pltpu.roll(back, HEAD_DIM, 1))
                else:
                    both_ways = jnp.where(low, pltpu.roll(ahead, HEAD_DIM, 1), back)
                update.append(both_ways.astype(BF16))
                span_row.append(head_rows(spans, f, g))
            span_row = jnp.concatenate(span_row, axis=1)

            @pl.when(j == x)
            def _():
                for m in range(HPG):
                    tr[m, x] = update[m]
                lr[x] = span_row

            @pl.when(j != x)
            def _():
                ls[j] = span_row
                for m in range(HPG):
                    ts[m, j] = update[m]
                log_copy(j).start()

        send_state(0, p)

        @pl.when(k > 0)
        def _():
            send_state(1, conv_pair(k - 1))

    send_state(1, conv_pair(pairs - 1))
    for u in range(2, chunks):
        @pl.loop(1, nx)
        def _(k):
            state_copy(u, lax.rem(x + k, nx)).start()

    @pl.loop(0, pairs)
    def _(p):
        cum_r, rate_r = cum_t[rows_of(p)], rate_t[rows_of(p)]
        cum_c = cum_r.T
        cv = state_conv(p, c_ref, co, xw + bw, PW + STATE)
        cc[:, b_cols(p)] = cv
        xv, bv = xc[:, x_cols(p)], bc[:, b_cols(p)]
        below, above = col_i < row_i, col_i > row_i
        products = []
        for q in range(2):
            scores = lax.dot_general(
                cv[:, q * STATE : (q + 1) * STATE], bv[:, q * STATE : (q + 1) * STATE],
                (((1,), (1,)), ((), ())), preferred_element_type=F32,
            )
            for i in range(HPG):
                f, g = HPG * q + i, 8 + HPG * q + i
                gap = jnp.where(
                    above,
                    cum_c[:, g : g + 1] - cum_r[g : g + 1],
                    cum_c[:, f : f + 1] - cum_r[f : f + 1],
                )
                r_f, r_b = rate_r[f : f + 1], rate_r[g : g + 1]
                coef = jnp.where(below, r_f, jnp.where(above, r_b, r_f + r_b))
                weights = (scores * jnp.exp(gap) * coef).astype(BF16)
                v = f // 2
                products.append(mm(weights, xv[:, 128 * v : 128 * (v + 1)]))
        yl[:, x_cols(p)] = jnp.concatenate(
            [jnp.where(low, products[2 * v], products[2 * v + 1]) for v in range(HPG)], axis=1
        )

    ry = half_rows // ny

    def part(row, m):
        return row[:, 128 * m : 128 * (m + 1)]

    def along_x(u):
        m, rows = u // 2, rows_in(u)

        @pl.loop(0, nx)
        def _(k):
            @pl.when(k != x)
            def _():
                if u == 0:
                    rcopy(ls.at[k], lr.at[k], l_s.at[k], l_r.at[k], partner).wait_recv()
                at = u * nx + k
                rcopy(
                    ts.at[m, k, rows], tr.at[m, k, rows], t_s.at[at], t_r.at[at], partner
                ).wait_recv()

        if u == 0:
            pcl[0] = jnp.zeros(pcl.shape[1:], F32)
            wide = jnp.concatenate([low] * HPG, axis=1)

            @pl.loop(0, nx)
            def _(k):
                pcl[k + 1] = pcl[k] + jnp.where(wide, lr[k], lr[nx - 1 - k])

            sl[...] = pcl[nx]

        pre[m, 0, rows] = jnp.zeros((half_rows, 128), F32)

        @pl.loop(0, nx)
        def _(k):
            d = jnp.where(low, part(lr[k], m), part(lr[nx - 1 - k], m))
            v = jnp.where(low, tr[m, k, rows].astype(F32), tr[m, nx - 1 - k, rows].astype(F32))
            pre[m, k + 1, rows] = pre[m, k, rows] * jnp.exp(d) + v

        ss[u] = pre[m, nx, rows].reshape(ny, ry, 128).astype(ss.dtype)

        @pl.loop(1, ny)
        def _(k):
            j = lax.rem(y + k, ny)
            if u == 0:
                rcopy(sl, ylr.at[y], sl_s.at[j], sl_r.at[y], {"y": j}).start()
            total_copy(u, j).start()

        yr[u, y] = ss[u, y]
        if u == 0:
            ylr[y] = sl[...]

    def total_copy(u, j):
        return rcopy(
            ss.at[u, j], yr.at[u, y], s_s.at[u * ny + j], s_r.at[u * ny + y], {"y": j}
        )

    def plane_copy(u, j):
        return rcopy(zq.at[u], zr.at[u, z], q_s.at[u * nz + j], q_r.at[u * nz + z], {"z": j})

    def incoming_copy(u, j):
        return rcopy(
            isd.at[u, j], ir.at[u, y], i_s.at[u * ny + j], i_r.at[u * ny + y], {"y": j}
        )

    def entry_copy(u, j):
        return rcopy(
            es.at[u // 2, j, rows_in(u)], er.at[u // 2, x, rows_in(u)],
            e_s.at[u * nx + j], e_r.at[u * nx + x], {"x": j},
        )

    def along_y(u):
        m = u // 2

        @pl.loop(1, ny)
        def _(k):
            j = lax.rem(y + k, ny)
            if u == 0:
                rcopy(sl, ylr.at[j], sl_s.at[j], sl_r.at[j], {"y": j}).wait_recv()
            at = u * ny + j
            rcopy(ss.at[u, j], yr.at[u, j], s_s.at[at], s_r.at[at], {"y": j}).wait_recv()

        if u == 0:
            ypcl[0] = jnp.zeros(ypcl.shape[1:], F32)
            wide = jnp.concatenate([low] * HPG, axis=1)

            @pl.loop(0, ny)
            def _(k):
                ypcl[k + 1] = ypcl[k] + jnp.where(wide, ylr[k], ylr[ny - 1 - k])

            zql[...] = ypcl[ny]

        running = jnp.zeros((ry, 128), F32)
        for k in range(ny):
            ypre[u, k] = running
            d = jnp.where(low, part(ylr[k], m), part(ylr[ny - 1 - k], m))
            v = jnp.where(low, yr[u, k].astype(F32), yr[u, ny - 1 - k].astype(F32))
            running = running * jnp.exp(d) + v
        zq[u] = running

        @pl.loop(1, nz)
        def _(k):
            j = lax.rem(z + k, nz)
            if u == 0:
                rcopy(zql, zlr.at[z], ql_s.at[j], ql_r.at[z], {"z": j}).start()
            plane_copy(u, j).start()

        zr[u, z] = zq[u]
        if u == 0:
            zlr[z] = zql[...]

    def along_z(u):
        m = u // 2

        @pl.loop(1, nz)
        def _(k):
            j = lax.rem(z + k, nz)
            if u == 0:
                rcopy(zql, zlr.at[j], ql_s.at[j], ql_r.at[j], {"z": j}).wait_recv()
            at = u * nz + j
            rcopy(zq.at[u], zr.at[u, j], q_s.at[at], q_r.at[at], {"z": j}).wait_recv()

        running = jnp.zeros((ry, 128), F32)
        entering = jnp.zeros((ry, 128), F32)
        wanted = jnp.where(low, z, nz - 1 - z)
        for k in range(nz):
            entering = jnp.where(wanted == k, running, entering)
            d = jnp.where(low, part(zlr[k], m), part(zlr[nz - 1 - k], m))
            v = jnp.where(low, zr[u, k], zr[u, nz - 1 - k])
            running = running * jnp.exp(d) + v

        def incoming(j):
            f = ypre[u, j] + jnp.exp(part(ypcl[j], m)) * entering
            b = ypre[u, ny - 1 - j] + jnp.exp(part(ypcl[ny - 1 - j], m)) * entering
            return jnp.where(low, f, b).astype(ir.dtype)

        @pl.loop(1, ny)
        def _(k):
            j = lax.rem(y + k, ny)
            isd[u, j] = incoming(j)
            incoming_copy(u, j).start()

        ir[u, y] = incoming(y)

    def back_along_x(u):
        m, rows = u // 2, rows_in(u)

        @pl.loop(1, ny)
        def _(k):
            j = lax.rem(y + k, ny)
            at = u * ny + j
            rcopy(isd.at[u, j], ir.at[u, j], i_s.at[at], i_r.at[at], {"y": j}).wait_recv()

        here = ir[u].astype(F32).reshape(half_rows, 128)

        def entry(j):
            f = pre[m, j, rows] + jnp.exp(part(pcl[j], m)) * here
            b = pre[m, nx - 1 - j, rows] + jnp.exp(part(pcl[nx - 1 - j], m)) * here
            return jnp.where(low, f, b).astype(BF16)

        @pl.loop(1, nx)
        def _(k):
            j = lax.rem(x + k, nx)
            es[m, j, rows] = entry(j)
            entry_copy(u, j).start()

        er[m, x, rows] = entry(x)

    def pair_at(k):
        away = (k + 1) // 2
        return lax.rem(x // 2 + jnp.where(lax.rem(k, 2) == 1, away, pairs - away), pairs)

    def await_entries(m, p):
        for q in range(2):
            j = 2 * p + q

            @pl.when(j != x)
            def _():
                for u in (2 * m, 2 * m + 1):
                    at, rows = u * nx + j, rows_in(u)
                    rcopy(
                        es.at[m, j, rows], er.at[m, j, rows], e_s.at[at], e_r.at[at], partner
                    ).wait_recv()

    def carried(m, p):
        cv = cc[:, b_cols(p)]
        decays = ecum_t[rows_of(p)].T
        for q in range(2):
            f, g = HPG * q + m, 8 + HPG * q + m
            v = mm(part(cv, q), er[m, 2 * p + q]) * head_rows(decays, f, g)
            v = v + pltpu.roll(v, HEAD_DIM, 1)
            mine = low if f % 2 == 0 else jnp.logical_not(low)
            cols = pl.ds(pl.multiple_of(PW * p + 128 * (f // 2), 128), 128)
            yl[:, cols] = yl[:, cols] + jnp.where(mine, v, 0.0)

    def free_sends():
        for copy in rate_copies + data_copies:
            copy.wait_send()

        @pl.when(target_exists)
        def _():
            for half in range(2):
                halo_copy(half).wait_send()

        @pl.loop(0, nx)
        def _(j):
            @pl.when(jnp.logical_not(weight_is_mine(j)))
            def _():
                weight_copy(j).wait_send()

            @pl.when(j != x)
            def _():
                log_copy(j).wait_send()
                for m in range(chunks):
                    state_copy(m, j).wait_send()

        @pl.loop(1, ny)
        def _(k):
            j = lax.rem(y + k, ny)
            rcopy(sl, ylr.at[y], sl_s.at[j], sl_r.at[y], {"y": j}).wait_send()
            for m in range(chunks):
                total_copy(m, j).wait_send()

        @pl.loop(1, nz)
        def _(k):
            j = lax.rem(z + k, nz)
            rcopy(zql, zlr.at[z], ql_s.at[j], ql_r.at[z], {"z": j}).wait_send()
            for m in range(chunks):
                plane_copy(m, j).wait_send()

    def carry(m):
        @pl.loop(0, pairs)
        def _(k):
            await_entries(m, pair_at(k))

        @pl.loop(0, pairs)
        def _(p):
            carried(m, p)

    arrival, stage = 2.9, 5.3
    steps = []
    for u in range(chunks):
        for k, step in enumerate((along_x, along_y, along_z, back_along_x)):
            steps.append((arrival * u + stage * k, step, u))
    steps.append((arrival + 3 * stage + 9.5, carry, 0))
    for _, step, u in sorted(steps, key=lambda t: t[0]):
        if step is back_along_x and u == chunks - 1:
            free_sends()
        step(u)

    @pl.loop(1, ny)
    def _(k):
        for m in range(chunks):
            incoming_copy(m, lax.rem(y + k, ny)).wait_send()

    carry(1)

    @pl.loop(1, nx)
    def _(k):
        for u in range(2 * (HPG - 1)):
            entry_copy(u, lax.rem(x + k, nx)).wait_send()

    block_r, block_c = iota((128, 128), 0) // HEAD_DIM, iota((128, 128), 1) // HEAD_DIM
    ones = (block_r == block_c).astype(BF16)

    def gate(mixed, cols):
        g = mixed.astype(F32) * zs[:, cols]
        sq = g * g
        hi = sq.astype(BF16)
        lo = (sq - hi.astype(F32)).astype(BF16)
        means = jnp.concatenate(
            [mm(part(hi, v), ones) + mm(part(lo, v), ones) for v in range(HPG)], axis=1
        ) * (1.0 / HEAD_DIM)
        normed = g * lax.rsqrt(means + 1e-06)
        out_ref[0, :, cols] = (normed * gs[:, cols]).astype(BF16)

    def own_cols(p, half):
        return pl.ds(pl.multiple_of(half * xw + PW * p, 128), PW)

    def mixed_copy(p):
        return rcopy(ys.at[p], yx.at[p], y_s.at[p], y_r.at[p], partner)

    def other_half(p):
        mixed_copy(p).wait_recv()
        gate(yx[p], own_cols(p, 1 - c))

    @pl.loop(0, pairs)
    def _(k):
        p = pair_at(k)
        await_entries(HPG - 1, p)
        carried(HPG - 1, p)
        mixed = yl[:, x_cols(p)]
        top, bottom = mixed[0:TOK].astype(BF16), mixed[TOK:n].astype(BF16)
        ys[p] = jnp.where(first, bottom, top)
        mixed_copy(p).start()
        gate(jnp.where(first, top, bottom), own_cols(p, c))

        @pl.when(k > 0)
        def _():
            other_half(pair_at(k - 1))

    other_half(pair_at(pairs - 1))

    @pl.loop(1, nx)
    def _(k):
        for u in (chunks - 2, chunks - 1):
            entry_copy(u, lax.rem(x + k, nx)).wait_send()

    @pl.loop(0, pairs)
    def _(p):
        mixed_copy(p).wait_send()


def local(sizes, *args):
    nx, ny, nz = sizes
    pairs = nx // 2
    xw, bw = pairs * PW, pairs * 2 * STATE
    n = 2 * TOK
    ry = STATE // 2 // ny
    chunks = 2 * HPG
    args = list(args)
    args[4:7] = [jnp.swapaxes(a, 1, 2) for a in args[4:7]]
    dma = pltpu.SemaphoreType.DMA
    vmem = pltpu.VMEM
    wide = PW + 4 * STATE
    scratch = [vmem(a.shape, a.dtype) for a in args] + [dma((len(args),))]
    scratch += [
        vmem((TOK, xw), BF16), vmem((TOK, bw), BF16), vmem((TOK, bw), BF16),
        vmem((3, args[4].shape[1], TOK), F32),
        vmem((2, 2, xw + 2 * bw), F32), vmem((2, 2, xw + 2 * bw), F32),
        vmem((TAPS, wide), BF16), vmem((nx, TAPS, wide), BF16),
        vmem((128, n), F32), vmem((128, n), F32), vmem((128, n), F32), vmem((128, n), F32),
        vmem((pairs, 1, 16), F32),
        vmem((n, xw), BF16), vmem((n, bw), BF16), vmem((n, bw), BF16), vmem((n, xw), F32),
        vmem((TOK, 2 * xw), F32), vmem((1, 2 * xw), F32),
        vmem((HPG, nx, STATE, 128), BF16), vmem((HPG, nx, STATE, 128), BF16),
        vmem((nx, 1, PW), F32), vmem((nx, 1, PW), F32),
        vmem((HPG, nx + 1, STATE, 128), F32), vmem((nx + 1, 1, PW), F32),
        vmem((chunks, ny, ry, 128), BF16), vmem((1, PW), F32),
        vmem((chunks, ny, ry, 128), BF16), vmem((ny, 1, PW), F32),
        vmem((chunks, ny, ry, 128), F32), vmem((ny + 1, 1, PW), F32),
        vmem((chunks, ry, 128), F32), vmem((1, PW), F32),
        vmem((chunks, nz, ry, 128), F32), vmem((nz, 1, PW), F32),
        vmem((chunks, ny, ry, 128), BF16), vmem((chunks, ny, ry, 128), BF16),
        vmem((HPG, nx, STATE, 128), BF16), vmem((HPG, nx, STATE, 128), BF16),
        vmem((pairs, TOK, PW), BF16), vmem((pairs, TOK, PW), BF16),
    ]
    hx, hy, hz = chunks * nx, chunks * ny, chunks * nz
    counts = [6, 6, 2, 2, nx, nx, hx, hx, nx, nx, hy, hy, ny, ny, hz, hz, nz, nz, hy, hy, hx, hx, pairs, pairs]
    scratch += [dma((k,)) for k in counts]
    return pl.pallas_call(
        functools.partial(kernel, sizes),
        out_shape=pltpu.VMEM(args[0].shape, BF16),
        in_specs=[pl.BlockSpec(memory_space=pltpu.HBM)] * len(args),
        out_specs=pl.BlockSpec(memory_space=pltpu.VMEM),
        scratch_shapes=scratch,
        compiler_params=pltpu.CompilerParams(
            collective_id=0, has_side_effects=True, vmem_limit_bytes=60 * 1024 * 1024
        ),
        name="mixer",
    )(*args)


def solution(mesh):
    sp, dp = mesh.shape["sp"], mesh.shape["dp"]
    nx = sp // 2
    ny = max(k for k in range(1, dp + 1) if dp % k == 0 and k * k <= dp)
    nz = dp // ny
    torus = Mesh(mesh.devices.reshape(nx, 2, nz, ny), ("x", "c", "z", "y"))
    rows = P(("z", "y"), ("x", "c"), None)
    cols = P(None, ("x", "c"))
    return jax.shard_map(
        functools.partial(local, (nx, ny, nz)),
        mesh=torus,
        in_specs=(rows,) * 7 + (cols,) * 5 + (P(),),
        out_specs=rows,
        check_vma=False,
    )
```

```python
import functools

import jax
import jax.numpy as jnp
from jax import lax
from jax.experimental import pallas as pl
from jax.experimental.pallas import tpu as pltpu
from jax.sharding import Mesh
from jax.sharding import PartitionSpec as P

MESH = pl.DeviceIdType.MESH
HEAD_DIM = 64
STATE = 128
TOK = 128
HPG = 3
TAPS = 4
GW = HPG * HEAD_DIM
PW = 2 * GW
HIGH = lax.Precision.HIGHEST
F32 = jnp.float32
BF16 = jnp.bfloat16


def iota(shape, dim):
    return lax.broadcasted_iota(jnp.int32, shape, dim)


def mm(a, b, precision=None):
    return jnp.dot(a, b, preferred_element_type=F32, precision=precision)


def rcopy(src, dst, send_sem, recv_sem, device):
    return pltpu.make_async_remote_copy(
        src_ref=src,
        dst_ref=dst,
        send_sem=send_sem,
        recv_sem=recv_sem,
        device_id=device,
        device_id_type=MESH,
    )


def head_rows(columns, f, b):
    low = iota((columns.shape[0], 128), 1) < HEAD_DIM
    return jnp.where(low, columns[:, f : f + 1], columns[:, b : b + 1])


def silu(t):
    h = 0.5 * t
    return h + h * jnp.tanh(h)


def conv_silu(own, other, before, after, taps, first):
    top, bottom = jnp.where(first, own, other), jnp.where(first, other, own)
    edge = iota((8, own.shape[1]), 0)
    ahead = jnp.where(edge == 6, before[0:1], jnp.where(edge == 7, before[1:2], 0.0))
    behind = jnp.where(edge == 0, after[0:1], 0.0)
    x = jnp.concatenate([ahead, top.astype(F32), bottom.astype(F32), behind], axis=0)
    rows = x.shape[0]
    inner = slice(8, rows - 8)
    m2, m1, p1 = (pltpu.roll(x, k, 0)[inner] for k in (2, 1, rows - 1))
    total = m2 * taps[0:1] + m1 * taps[1:2] + x[inner] * taps[2:3] + p1 * taps[3:4]
    return silu(total).astype(BF16)


def three(v):
    hi = v.astype(BF16)
    left = v - hi.astype(F32)
    mid = left.astype(BF16)
    return hi, mid, (left - mid.astype(F32)).astype(BF16)


def kernel(
    sizes,
    x_in, b_in, c_in, z_in, ra_in, rr_in, rf_in,
    wx_in, wb_in, wc_in, off_in, spd_in, gain_in,
    out_ref,
    x_ref, b_ref, c_ref, z_ref, ra_ref, rr_ref, rf_ref,
    wx_ref, wb_ref, wc_ref, off_ref, spd_ref, gain_ref, in_s,
    xo, bo, co, ro, hs, hr, ws, wr,
    cum_t, rate_t, fac_t, ecum_t, span_row_of, bts,
    xc, bc, cc, yl, zs, gs,
    ts, tr, ls, lr, pre, pcl,
    ss, sl, yr, ylr, ypre, ypcl,
    zq, zql, zr, zlr,
    isd, ir, es, er,
    ys, yx,
    d_s, d_r, h_s, h_r, w_s, w_r,
    t_s, t_r, l_s, l_r, s_s, s_r, sl_s, sl_r,
    q_s, q_r, ql_s, ql_r, i_s, i_r, e_s, e_r, y_s, y_r,
):
    sources = (
        wx_in, wb_in, wc_in, off_in, spd_in, x_in, b_in, c_in, ra_in, rr_in, rf_in, z_in, gain_in
    )
    places = (
        wx_ref, wb_ref, wc_ref, off_ref, spd_ref, x_ref, b_ref, c_ref, ra_ref, rr_ref, rf_ref,
        z_ref, gain_ref,
    )
    loads = [
        pltpu.make_async_copy(source, place, in_s.at[k])
        for k, (source, place) in enumerate(zip(sources, places))
    ]
    for load in loads:
        load.start()

    nx, ny, nz = sizes
    pairs = nx // 2
    xw, bw = pairs * PW, pairs * 2 * STATE
    x, c, z, y = (lax.axis_index(n) for n in ("x", "c", "z", "y"))
    first = c == 0
    partner = {"c": 1 - c}
    lin = (z * ny + y) * nx + x
    total_chips = nx * ny * nz
    has_prev, has_next = lin > 0, lin < total_chips - 1

    def chip(at):
        at = lax.rem(at + total_chips, total_chips)
        rest = at // nx
        return {"x": lax.rem(at, nx), "y": lax.rem(rest, ny), "z": rest // ny}

    target_exists = jnp.logical_or(
        jnp.logical_and(first, has_prev), jnp.logical_and(jnp.logical_not(first), has_next)
    )
    target = chip(jnp.where(first, lin - 1, lin + 1))

    barrier = pltpu.get_barrier_semaphore()

    def greet(device):
        pl.semaphore_signal(barrier, inc=1, device_id=device, device_id_type=MESH)

    greet(partner)

    @pl.loop(1, nx)
    def _(k):
        at = lax.rem(x + k, nx)
        greet({"x": at})
        greet({"x": at, "c": 1 - c})

    @pl.loop(1, ny)
    def _(k):
        greet({"y": lax.rem(y + k, ny)})

    @pl.loop(1, nz)
    def _(k):
        greet({"z": lax.rem(z + k, nz)})

    @pl.when(has_prev)
    def _():
        greet({**chip(lin - 1), "c": 1})

    @pl.when(has_next)
    def _():
        greet({**chip(lin + 1), "c": 0})

    for load in loads[:5]:
        load.wait()

    group = 2 * x + c
    slot = lax.rem(group, nx)
    parity = lax.rem(slot, 2)
    place = (iota((GW, PW), 1) == iota((GW, PW), 0) + GW * parity).astype(BF16)
    ws[:, 0:PW] = mm(wx_ref[...], place).astype(BF16)
    ws[:, PW : PW + STATE] = wb_ref[...]
    ws[:, PW + STATE : PW + 2 * STATE] = wc_ref[...]
    lane = iota((1, 128), 1)
    base = 16 * (slot // 2) + HPG * parity
    tap = iota((TAPS, 128), 0)
    for k, ref in enumerate((off_ref, spd_ref)):
        row = jnp.zeros((1, 128), F32)
        for d in range(2):
            for i in range(HPG):
                row = jnp.where(lane == base + 8 * d + i, ref[d : d + 1, i : i + 1], row)
        parts = [v.astype(F32) for v in three(row)]
        rows = jnp.where(
            tap == 0, parts[0], jnp.where(tap == 1, parts[1], jnp.where(tap == 2, parts[2], 0.0))
        )
        lo = PW + (2 + k) * STATE
        ws[:, lo : lo + STATE] = rows.astype(BF16)

    for load in loads[5:8]:
        load.wait()

    at = 0
    for ref, width in ((x_ref, xw), (b_ref, bw), (c_ref, bw)):
        for half in range(2):
            cols = pl.ds(half * width, width)
            last = ref[0, TOK - 16 : TOK, cols].astype(F32)[8:16]
            start = ref[0, 0:16, cols].astype(F32)[0:8]
            rows = jnp.where(first, start, pltpu.roll(last, 2, 0))
            hs[half, :, at : at + width] = rows[0:2]
        at += width

    @pl.when(jnp.logical_not(has_prev))
    def _():
        hr[0] = jnp.zeros(hr.shape[1:], F32)

    @pl.when(jnp.logical_not(has_next))
    def _():
        hr[1] = jnp.zeros(hr.shape[1:], F32)

    for load in loads[8:]:
        load.wait()

    expected = 1 + 2 * (nx - 1) + (ny - 1) + (nz - 1)
    pl.semaphore_wait(barrier, expected + jnp.where(target_exists, 2, 0))

    def half_of(ref, width, half):
        return ref.at[0, :, pl.ds(pl.multiple_of(half * width, 128), width)]

    rate_copies = [
        rcopy(ref.at[0], ro.at[k], d_s.at[k], d_r.at[k], partner)
        for k, ref in enumerate((ra_ref, rr_ref, rf_ref))
    ]
    data_copies = [
        rcopy(half_of(ref, width, 1 - c), dst, d_s.at[3 + k], d_r.at[3 + k], partner)
        for k, (ref, width, dst) in enumerate(((x_ref, xw, xo), (b_ref, bw, bo), (c_ref, bw, co)))
    ]

    to_core = group // nx

    def weight_copy(j):
        return rcopy(ws, wr.at[slot], w_s.at[j], w_r.at[slot], {"x": j, "c": to_core})

    def weight_is_mine(j):
        return jnp.logical_and(j == x, to_core == c)

    @pl.loop(0, nx)
    def _(k):
        j = lax.rem(x + nx // 2 + k, nx)

        @pl.when(jnp.logical_not(weight_is_mine(j)))
        def _():
            weight_copy(j).start()

    @pl.when(to_core == c)
    def _():
        wr[slot] = ws[...]

    for copy in rate_copies:
        copy.start()

    def halo_copy(half):
        return rcopy(
            hs.at[half], hr.at[1 - c], h_s.at[half], h_r.at[1 - c], {**target, "c": half}
        )

    @pl.when(target_exists)
    def _():
        for half in range(2):
            halo_copy(half).start()

    for copy in data_copies:
        copy.start()

    for copy in rate_copies:
        copy.wait_recv()

    n = 2 * TOK
    heads = ra_ref.shape[1]
    lanes, head = iota((128, heads), 0), iota((128, heads), 1)
    pair, rest = lanes // 16, lax.rem(lanes, 16)
    inside = lax.rem(rest, 8)
    valid = jnp.logical_and(inside < 6, pair < pairs)
    valid = jnp.logical_and(valid, head == 6 * pairs * c + 6 * pair + inside)
    pick_f = jnp.logical_and(valid, rest < 8).astype(F32)
    pick_b = jnp.logical_and(valid, rest >= 8).astype(F32)

    def both(ref, k):
        own, other = ref[0], ro[k]
        return jnp.concatenate(
            [jnp.where(first, own, other), jnp.where(first, other, own)], axis=1
        )

    raw = mm(pick_f, both(ra_ref, 0), HIGH) + mm(pick_b, both(rr_ref, 1), HIGH)
    fading = mm(pick_f + pick_b, both(rf_ref, 2), HIGH)

    def gate_cols(k):
        return pl.ds(pl.multiple_of(k * PW, 128), PW)

    for k in range(2 * xw // 128):
        cols = slice(128 * k, 128 * (k + 1))
        gs[:, cols] = gain_ref[cols].astype(F32).reshape(1, 128)

    @pl.loop(0, 2 * pairs)
    def _(k):
        zz = z_ref[0, :, gate_cols(k)].astype(F32)
        zs[:, gate_cols(k)] = silu(zz)

    @pl.loop(0, nx)
    def _(j):
        @pl.when(jnp.logical_not(nx * c + j == group))
        def _():
            rcopy(ws, wr.at[j], w_s.at[j], w_r.at[j], partner).wait_recv()

    def summed(lo):
        row = jnp.zeros((1, 128), F32)
        for j in range(nx):
            v = wr[j, :, lo : lo + 128].astype(F32)
            row = row + ((v[0:1] + v[1:2]) + v[2:3])
        return jnp.broadcast_to(row, (8, 128)).T[:, 0:1]

    offset, speed = summed(PW + 2 * STATE), summed(PW + 3 * STATE)
    pre_rate = raw + offset
    rate = jnp.maximum(pre_rate, 0.0) + jnp.log1p(jnp.exp(-jnp.abs(pre_rate)))
    log = fading - jnp.exp(speed) * rate
    row_i, col_i = iota((n, n), 0), iota((n, n), 1)
    forward = lax.rem(iota((128, 1), 0), 16) < 8
    upper, lower = (row_i <= col_i).astype(BF16), (row_i >= col_i).astype(BF16)
    parts = three(log)
    cum = jnp.where(
        forward,
        (mm(parts[2], upper) + mm(parts[1], upper)) + mm(parts[0], upper),
        (mm(parts[2], lower) + mm(parts[1], lower)) + mm(parts[0], lower),
    )
    span = jnp.where(forward, cum[:, n - 1 : n], cum[:, 0:1])
    span_line = jnp.broadcast_to(span, (128, 128)).T[0:1]
    for p in range(pairs):
        span_row_of[p] = span_line[:, 16 * p : 16 * (p + 1)]
    cum_t[...] = cum
    rate_t[...] = rate
    fac_t[...] = rate * jnp.exp(span - cum)
    ecum_t[...] = jnp.exp(cum)

    @pl.when(has_prev)
    def _():
        rcopy(hs.at[0], hr.at[0], h_s.at[0], h_r.at[0], partner).wait_recv()

    @pl.when(has_next)
    def _():
        rcopy(hs.at[0], hr.at[1], h_s.at[0], h_r.at[1], partner).wait_recv()

    for copy in data_copies:
        copy.wait_recv()

    low = iota((1, 128), 1) < HEAD_DIM

    def rows_of(p):
        return pl.ds(pl.multiple_of(16 * p, 16), 16)

    def x_cols(p):
        return pl.ds(pl.multiple_of(PW * p, 128), PW)

    def b_cols(p):
        return pl.ds(pl.multiple_of(2 * STATE * p, 128), 2 * STATE)

    half_rows = STATE // 2
    chunks = 2 * HPG

    def rows_in(u):
        return pl.ds(half_rows * (u % 2), half_rows)

    def state_copy(u, j):
        return rcopy(
            ts.at[u // 2, j, rows_in(u)], tr.at[u // 2, x, rows_in(u)],
            t_s.at[u * nx + j], t_r.at[u * nx + x], {"x": j},
        )

    def conv_pair(k):
        return lax.rem(x // 2 + 1 + k, pairs)

    def log_copy(j):
        return rcopy(ls.at[j], lr.at[x], l_s.at[j], l_r.at[x], {"x": j})

    def state_conv(p, own, other, at, lo):
        start = pl.multiple_of(2 * STATE * p, 128)
        taps = jnp.concatenate(
            [wr[2 * p, :, lo : lo + STATE], wr[2 * p + 1, :, lo : lo + STATE]], axis=1
        ).astype(F32)
        cols_in = pl.ds(pl.multiple_of(c * bw + start, 128), 2 * STATE)
        cols_h = pl.ds(pl.multiple_of(at + start, 128), 2 * STATE)
        return conv_silu(
            own[0, :, cols_in], other[:, b_cols(p)], hr[0, :, cols_h], hr[1, :, cols_h],
            taps, first,
        )

    def own_state(p, q, i, bt):
        j, factors = 2 * p + q, fac_t[rows_of(p)]
        f, g = HPG * q + i, 8 + HPG * q + i
        cols = pl.ds(pl.multiple_of(PW * p + 128 * (f // 2), 128), 128)
        v = xc[:, cols]
        ahead = mm((bt * factors[f : f + 1]).astype(BF16), v)
        back = mm((bt * factors[g : g + 1]).astype(BF16), v)
        if f % 2 == 0:
            update = jnp.where(low, ahead, pltpu.roll(back, HEAD_DIM, 1))
        else:
            update = jnp.where(low, pltpu.roll(ahead, HEAD_DIM, 1), back)
        ts[i, j] = update.astype(BF16)

    @pl.loop(0, pairs)
    def _(k):
        p = conv_pair(k)
        w0, w1 = wr[2 * p].astype(F32), wr[2 * p + 1].astype(F32)
        cols, start = x_cols(p), pl.multiple_of(PW * p, 128)
        x_cols_in = pl.ds(pl.multiple_of(c * xw + start, 128), PW)
        xv = conv_silu(
            x_ref[0, :, x_cols_in], xo[:, cols], hr[0, :, cols], hr[1, :, cols],
            w0[:, 0:PW] + w1[:, 0:PW], first,
        )
        xc[:, cols] = xv
        bv = state_conv(p, b_ref, bo, xw, PW)
        bc[:, b_cols(p)] = bv
        bf = bv.astype(F32)
        for q in range(2):
            bt = bf[:, q * STATE : (q + 1) * STATE].T
            bts[2 * p + q] = bt
            own_state(p, q, 0, bt)
            ls[2 * p + q] = jnp.concatenate(
                [
                    head_rows(span_row_of[p], HPG * q + i, 8 + HPG * q + i)
                    for i in range(HPG)
                ],
                axis=1,
            )
        for q in range(2):
            @pl.when(2 * p + q != x)
            def _():
                log_copy(2 * p + q).start()
                state_copy(0, 2 * p + q).start()

    lr[x] = ls[x]

    def send_chunk(u):
        @pl.loop(1, nx)
        def _(k):
            state_copy(u, lax.rem(x + k, nx)).start()

    send_chunk(1)

    @pl.loop(0, pairs)
    def _(k):
        p = conv_pair(k)
        for q in range(2):
            bt = bts[2 * p + q]
            for i in range(1, HPG):
                own_state(p, q, i, bt)

    for u in range(2, chunks):
        send_chunk(u)
    for m in range(HPG):
        tr[m, x] = ts[m, x]

    def inside_chip(p):
        cum_r, rate_r = cum_t[rows_of(p)], rate_t[rows_of(p)]
        cum_c = cum_r.T
        cv = state_conv(p, c_ref, co, xw + bw, PW + STATE)
        cc[:, b_cols(p)] = cv
        xv, bv = xc[:, x_cols(p)], bc[:, b_cols(p)]
        below, above = col_i < row_i, col_i > row_i
        products = []
        for q in range(2):
            scores = lax.dot_general(
                cv[:, q * STATE : (q + 1) * STATE], bv[:, q * STATE : (q + 1) * STATE],
                (((1,), (1,)), ((), ())), preferred_element_type=F32,
            )
            for i in range(HPG):
                f, g = HPG * q + i, 8 + HPG * q + i
                gap = jnp.where(
                    above,
                    cum_c[:, g : g + 1] - cum_r[g : g + 1],
                    cum_c[:, f : f + 1] - cum_r[f : f + 1],
                )
                r_f, r_b = rate_r[f : f + 1], rate_r[g : g + 1]
                coef = jnp.where(below, r_f, jnp.where(above, r_b, r_f + r_b))
                weights = (scores * jnp.exp(gap) * coef).astype(BF16)
                v = f // 2
                products.append(mm(weights, xv[:, 128 * v : 128 * (v + 1)]))
        yl[:, x_cols(p)] = jnp.concatenate(
            [jnp.where(low, products[2 * v], products[2 * v + 1]) for v in range(HPG)], axis=1
        )

    ry = half_rows // ny

    def part(row, m):
        return row[:, 128 * m : 128 * (m + 1)]

    def along_x(u):
        m, rows = u // 2, rows_in(u)

        @pl.loop(0, nx)
        def _(k):
            @pl.when(k != x)
            def _():
                if u == 0:
                    rcopy(ls.at[k], lr.at[k], l_s.at[k], l_r.at[k], partner).wait_recv()
                at = u * nx + k
                rcopy(
                    ts.at[m, k, rows], tr.at[m, k, rows], t_s.at[at], t_r.at[at], partner
                ).wait_recv()

        if u == 0:
            pcl[0] = jnp.zeros(pcl.shape[1:], F32)
            wide = jnp.concatenate([low] * HPG, axis=1)

            @pl.loop(0, nx)
            def _(k):
                pcl[k + 1] = pcl[k] + jnp.where(wide, lr[k], lr[nx - 1 - k])

            sl[...] = pcl[nx]

        pre[m, 0, rows] = jnp.zeros((half_rows, 128), F32)

        @pl.loop(0, nx)
        def _(k):
            d = jnp.where(low, part(lr[k], m), part(lr[nx - 1 - k], m))
            v = jnp.where(low, tr[m, k, rows].astype(F32), tr[m, nx - 1 - k, rows].astype(F32))
            pre[m, k + 1, rows] = pre[m, k, rows] * jnp.exp(d) + v

        ss[u] = pre[m, nx, rows].reshape(ny, ry, 128).astype(ss.dtype)

        @pl.loop(1, ny)
        def _(k):
            j = lax.rem(y + k, ny)
            if u == 0:
                rcopy(sl, ylr.at[y], sl_s.at[j], sl_r.at[y], {"y": j}).start()
            total_copy(u, j).start()

        yr[u, y] = ss[u, y]
        if u == 0:
            ylr[y] = sl[...]

    def total_copy(u, j):
        return rcopy(
            ss.at[u, j], yr.at[u, y], s_s.at[u * ny + j], s_r.at[u * ny + y], {"y": j}
        )

    def plane_copy(u, j):
        return rcopy(zq.at[u], zr.at[u, z], q_s.at[u * nz + j], q_r.at[u * nz + z], {"z": j})

    def incoming_copy(u, j):
        return rcopy(
            isd.at[u, j], ir.at[u, y], i_s.at[u * ny + j], i_r.at[u * ny + y], {"y": j}
        )

    def entry_copy(u, j):
        return rcopy(
            es.at[u // 2, j, rows_in(u)], er.at[u // 2, x, rows_in(u)],
            e_s.at[u * nx + j], e_r.at[u * nx + x], {"x": j},
        )

    def along_y(u):
        m = u // 2

        @pl.loop(1, ny)
        def _(k):
            j = lax.rem(y + k, ny)
            if u == 0:
                rcopy(sl, ylr.at[j], sl_s.at[j], sl_r.at[j], {"y": j}).wait_recv()
            at = u * ny + j
            rcopy(ss.at[u, j], yr.at[u, j], s_s.at[at], s_r.at[at], {"y": j}).wait_recv()

        if u == 0:
            ypcl[0] = jnp.zeros(ypcl.shape[1:], F32)
            wide = jnp.concatenate([low] * HPG, axis=1)

            @pl.loop(0, ny)
            def _(k):
                ypcl[k + 1] = ypcl[k] + jnp.where(wide, ylr[k], ylr[ny - 1 - k])

            zql[...] = ypcl[ny]

        running = jnp.zeros((ry, 128), F32)
        for k in range(ny):
            ypre[u, k] = running
            d = jnp.where(low, part(ylr[k], m), part(ylr[ny - 1 - k], m))
            v = jnp.where(low, yr[u, k].astype(F32), yr[u, ny - 1 - k].astype(F32))
            running = running * jnp.exp(d) + v
        zq[u] = running

        @pl.loop(1, nz)
        def _(k):
            j = lax.rem(z + k, nz)
            if u == 0:
                rcopy(zql, zlr.at[z], ql_s.at[j], ql_r.at[z], {"z": j}).start()
            plane_copy(u, j).start()

        zr[u, z] = zq[u]
        if u == 0:
            zlr[z] = zql[...]

    def along_z(u):
        m = u // 2

        @pl.loop(1, nz)
        def _(k):
            j = lax.rem(z + k, nz)
            if u == 0:
                rcopy(zql, zlr.at[j], ql_s.at[j], ql_r.at[j], {"z": j}).wait_recv()
            at = u * nz + j
            rcopy(zq.at[u], zr.at[u, j], q_s.at[at], q_r.at[at], {"z": j}).wait_recv()

        running = jnp.zeros((ry, 128), F32)
        entering = jnp.zeros((ry, 128), F32)
        wanted = jnp.where(low, z, nz - 1 - z)
        for k in range(nz):
            entering = jnp.where(wanted == k, running, entering)
            d = jnp.where(low, part(zlr[k], m), part(zlr[nz - 1 - k], m))
            v = jnp.where(low, zr[u, k], zr[u, nz - 1 - k])
            running = running * jnp.exp(d) + v

        def incoming(j):
            f = ypre[u, j] + jnp.exp(part(ypcl[j], m)) * entering
            b = ypre[u, ny - 1 - j] + jnp.exp(part(ypcl[ny - 1 - j], m)) * entering
            return jnp.where(low, f, b).astype(ir.dtype)

        @pl.loop(1, ny)
        def _(k):
            j = lax.rem(y + k, ny)
            isd[u, j] = incoming(j)
            incoming_copy(u, j).start()

        ir[u, y] = incoming(y)

    def back_along_x(u):
        m, rows = u // 2, rows_in(u)

        @pl.loop(1, ny)
        def _(k):
            j = lax.rem(y + k, ny)
            at = u * ny + j
            rcopy(isd.at[u, j], ir.at[u, j], i_s.at[at], i_r.at[at], {"y": j}).wait_recv()

        here = ir[u].astype(F32).reshape(half_rows, 128)

        def entry(j):
            f = pre[m, j, rows] + jnp.exp(part(pcl[j], m)) * here
            b = pre[m, nx - 1 - j, rows] + jnp.exp(part(pcl[nx - 1 - j], m)) * here
            return jnp.where(low, f, b).astype(BF16)

        @pl.loop(1, nx)
        def _(k):
            j = lax.rem(x + k, nx)
            es[m, j, rows] = entry(j)
            entry_copy(u, j).start()

        er[m, x, rows] = entry(x)

    def pair_at(k):
        away = (k + 1) // 2
        return lax.rem(x // 2 + jnp.where(lax.rem(k, 2) == 1, away, pairs - away), pairs)

    def await_entries(m, p):
        for q in range(2):
            j = 2 * p + q

            @pl.when(j != x)
            def _():
                for u in (2 * m, 2 * m + 1):
                    at, rows = u * nx + j, rows_in(u)
                    rcopy(
                        es.at[m, j, rows], er.at[m, j, rows], e_s.at[at], e_r.at[at], partner
                    ).wait_recv()

    def carried(m, p):
        cv = cc[:, b_cols(p)]
        decays = ecum_t[rows_of(p)].T
        for q in range(2):
            f, g = HPG * q + m, 8 + HPG * q + m
            v = mm(part(cv, q), er[m, 2 * p + q]) * head_rows(decays, f, g)
            v = v + pltpu.roll(v, HEAD_DIM, 1)
            mine = low if f % 2 == 0 else jnp.logical_not(low)
            cols = pl.ds(pl.multiple_of(PW * p + 128 * (f // 2), 128), 128)
            yl[:, cols] = yl[:, cols] + jnp.where(mine, v, 0.0)

    def free_sends():
        for copy in rate_copies + data_copies:
            copy.wait_send()

        @pl.when(target_exists)
        def _():
            for half in range(2):
                halo_copy(half).wait_send()

        @pl.loop(0, nx)
        def _(j):
            @pl.when(jnp.logical_not(weight_is_mine(j)))
            def _():
                weight_copy(j).wait_send()

            @pl.when(j != x)
            def _():
                log_copy(j).wait_send()
                for m in range(chunks):
                    state_copy(m, j).wait_send()

        @pl.loop(1, ny)
        def _(k):
            j = lax.rem(y + k, ny)
            rcopy(sl, ylr.at[y], sl_s.at[j], sl_r.at[y], {"y": j}).wait_send()
            for m in range(chunks):
                total_copy(m, j).wait_send()

        @pl.loop(1, nz)
        def _(k):
            j = lax.rem(z + k, nz)
            rcopy(zql, zlr.at[z], ql_s.at[j], ql_r.at[z], {"z": j}).wait_send()
            for m in range(chunks):
                plane_copy(m, j).wait_send()

    def carry(m):
        @pl.loop(0, pairs)
        def _(k):
            await_entries(m, pair_at(k))

        @pl.loop(0, pairs)
        def _(p):
            carried(m, p)

    arrival, stage = 2.9, 5.3
    early = (pairs + 1) // 2
    steps = []

    @pl.loop(0, early)
    def _(p):
        inside_chip(p)

    for k, p in enumerate(range(early, pairs)):
        steps.append((0.4 + arrival * k, inside_chip, p))
    for u in range(chunks):
        for k, step in enumerate((along_x, along_y, along_z, back_along_x)):
            steps.append((arrival * u + stage * k, step, u))
    steps.append((arrival + 3 * stage + 9.5, carry, 0))
    for _, step, u in sorted(steps, key=lambda t: t[0]):
        if step is back_along_x and u == chunks - 1:
            free_sends()
        step(u)

    @pl.loop(1, ny)
    def _(k):
        for m in range(chunks):
            incoming_copy(m, lax.rem(y + k, ny)).wait_send()

    carry(1)

    @pl.loop(1, nx)
    def _(k):
        for u in range(2 * (HPG - 1)):
            entry_copy(u, lax.rem(x + k, nx)).wait_send()

    block_r, block_c = iota((128, 128), 0) // HEAD_DIM, iota((128, 128), 1) // HEAD_DIM
    ones = (block_r == block_c).astype(BF16)

    def gate(mixed, cols):
        g = mixed.astype(F32) * zs[:, cols]
        sq = g * g
        hi = sq.astype(BF16)
        lo = (sq - hi.astype(F32)).astype(BF16)
        means = jnp.concatenate(
            [mm(part(hi, v), ones) + mm(part(lo, v), ones) for v in range(HPG)], axis=1
        ) * (1.0 / HEAD_DIM)
        normed = g * lax.rsqrt(means + 1e-06)
        out_ref[0, :, cols] = (normed * gs[:, cols]).astype(BF16)

    def own_cols(p, half):
        return pl.ds(pl.multiple_of(half * xw + PW * p, 128), PW)

    def mixed_copy(p):
        return rcopy(ys.at[p], yx.at[p], y_s.at[p], y_r.at[p], partner)

    def other_half(p):
        mixed_copy(p).wait_recv()
        gate(yx[p], own_cols(p, 1 - c))

    @pl.loop(0, pairs)
    def _(k):
        p = pair_at(k)
        await_entries(HPG - 1, p)
        carried(HPG - 1, p)
        mixed = yl[:, x_cols(p)]
        top, bottom = mixed[0:TOK].astype(BF16), mixed[TOK:n].astype(BF16)
        ys[p] = jnp.where(first, bottom, top)
        mixed_copy(p).start()
        gate(jnp.where(first, top, bottom), own_cols(p, c))

        @pl.when(k > 0)
        def _():
            other_half(pair_at(k - 1))

    other_half(pair_at(pairs - 1))

    @pl.loop(1, nx)
    def _(k):
        for u in (chunks - 2, chunks - 1):
            entry_copy(u, lax.rem(x + k, nx)).wait_send()

    @pl.loop(0, pairs)
    def _(p):
        mixed_copy(p).wait_send()


def local(sizes, *args):
    nx, ny, nz = sizes
    pairs = nx // 2
    xw, bw = pairs * PW, pairs * 2 * STATE
    n = 2 * TOK
    ry = STATE // 2 // ny
    chunks = 2 * HPG
    args = list(args)
    args[4:7] = [jnp.swapaxes(a, 1, 2) for a in args[4:7]]
    dma = pltpu.SemaphoreType.DMA
    vmem = pltpu.VMEM
    wide = PW + 4 * STATE
    scratch = [vmem(a.shape, a.dtype) for a in args] + [dma((len(args),))]
    scratch += [
        vmem((TOK, xw), BF16), vmem((TOK, bw), BF16), vmem((TOK, bw), BF16),
        vmem((3, args[4].shape[1], TOK), F32),
        vmem((2, 2, xw + 2 * bw), F32), vmem((2, 2, xw + 2 * bw), F32),
        vmem((TAPS, wide), BF16), vmem((nx, TAPS, wide), BF16),
        vmem((128, n), F32), vmem((128, n), F32), vmem((128, n), F32), vmem((128, n), F32),
        vmem((pairs, 1, 16), F32), vmem((nx, STATE, n), F32),
        vmem((n, xw), BF16), vmem((n, bw), BF16), vmem((n, bw), BF16), vmem((n, xw), F32),
        vmem((TOK, 2 * xw), F32), vmem((1, 2 * xw), F32),
        vmem((HPG, nx, STATE, 128), BF16), vmem((HPG, nx, STATE, 128), BF16),
        vmem((nx, 1, PW), F32), vmem((nx, 1, PW), F32),
        vmem((HPG, nx + 1, STATE, 128), F32), vmem((nx + 1, 1, PW), F32),
        vmem((chunks, ny, ry, 128), BF16), vmem((1, PW), F32),
        vmem((chunks, ny, ry, 128), BF16), vmem((ny, 1, PW), F32),
        vmem((chunks, ny, ry, 128), F32), vmem((ny + 1, 1, PW), F32),
        vmem((chunks, ry, 128), F32), vmem((1, PW), F32),
        vmem((chunks, nz, ry, 128), F32), vmem((nz, 1, PW), F32),
        vmem((chunks, ny, ry, 128), BF16), vmem((chunks, ny, ry, 128), BF16),
        vmem((HPG, nx, STATE, 128), BF16), vmem((HPG, nx, STATE, 128), BF16),
        vmem((pairs, TOK, PW), BF16), vmem((pairs, TOK, PW), BF16),
    ]
    hx, hy, hz = chunks * nx, chunks * ny, chunks * nz
    counts = [6, 6, 2, 2, nx, nx, hx, hx, nx, nx, hy, hy, ny, ny, hz, hz, nz, nz, hy, hy, hx, hx, pairs, pairs]
    scratch += [dma((k,)) for k in counts]
    return pl.pallas_call(
        functools.partial(kernel, sizes),
        out_shape=pltpu.VMEM(args[0].shape, BF16),
        in_specs=[pl.BlockSpec(memory_space=pltpu.HBM)] * len(args),
        out_specs=pl.BlockSpec(memory_space=pltpu.VMEM),
        scratch_shapes=scratch,
        compiler_params=pltpu.CompilerParams(
            collective_id=0, has_side_effects=True, vmem_limit_bytes=60 * 1024 * 1024
        ),
        name="mixer",
    )(*args)


def solution(mesh):
    sp, dp = mesh.shape["sp"], mesh.shape["dp"]
    nx = sp // 2
    ny = max(k for k in range(1, dp + 1) if dp % k == 0 and k * k <= dp)
    nz = dp // ny
    torus = Mesh(mesh.devices.reshape(nx, 2, nz, ny), ("x", "c", "z", "y"))
    rows = P(("z", "y"), ("x", "c"), None)
    cols = P(None, ("x", "c"))
    return jax.shard_map(
        functools.partial(local, (nx, ny, nz)),
        mesh=torus,
        in_specs=(rows,) * 7 + (cols,) * 5 + (P(),),
        out_specs=rows,
        check_vma=False,
    )
```
